32 devices in a mesh: grp: 2 (over y), fs: 8 (over z, core), tp: 2 (over x).
Axes of the slice: x: 2, y: 2, z: 4, core: 2. Of those that a mesh axis runs over, the one named last changes fastest.
Arguments:
- prompt: bfloat16 [6144, 2048], P(('grp', 'fs')), parts along dimension 0, may hold values from -6 to 6
- routes: int32 [6144, 4], P(('grp', 'fs')), parts along dimension 0, may hold values from 0 to 7, all different within a row; in each aligned block of 384 rows (0 to 383, 384 to 767, ...) at most 240 rows name the same one
- route_weight: float32 [6144, 4], P(('grp', 'fs')), parts along dimension 0, may hold values from 0.2 to 1
- norm_gain: float32 [2048], P('fs'), may hold values from 0.1 to 1.9
- gate_train: float32 [8, 2048, 1024], P(None, 'fs', 'tp'), may hold values from -0.4 to 0.4
- up_train: float32 [8, 2048, 1024], P(None, 'fs', 'tp'), may hold values from -0.4 to 0.4
- down_train: float32 [8, 1024, 2048], P(None, 'fs', 'tp'), may hold values from -0.07 to 0.07
Outputs:
- gate_serve: bfloat16 [16, 2048, 1024], P(('grp', 'fs'), None, 'tp'), parts along dimension 0
- up_serve: bfloat16 [16, 2048, 1024], P(('grp', 'fs'), None, 'tp'), parts along dimension 0
- down_serve: bfloat16 [16, 1024, 2048], P(('grp', 'fs'), 'tp'), parts along dimension 0
- mixed: bfloat16 [6144, 2048], P(('grp', 'fs'), 'tp'), parts along dimension 0
The draws below stay inside these ranges and needn't reach their ends.
There are 2 independent parts, one for each index of `grp`. The reference program is written for one: setup_inputs(seed, part) draws one part's arguments, and reference() takes and returns one part's arrays. A program takes and returns all parts, laid end to end along the dimension named above; an argument that names none is the same for every part. Nothing has to cross between parts.
Inputs may be any that keep to these rules, and one draw needn't show every extreme that they name: `routes`: each row names 4 different experts. Among the rows of one index of fs no expert is named more than 240 times, a bound that some block reaches on some index.
All inputs are finite; a program needn't handle non-finite values.
Results may differ from the reference program's by a relative error of at most 0.012.
Values may be sent and summed in bfloat16 or wider, within the bound.
A program may use at most 128 MiB of HBM per device.

```python
import math
import jax
import jax.numpy as jnp
import numpy as np
from jax import lax

D = 2048
FF = 1024
TOP = 4
TOK_DEV = 384
EXPERTS = 8
CAP = 240
TOKENS = 3072
N_FS = 8
N_TP = 2


def shard_levels(stream_key, extent, shards, least, top_value):
    loudness, own = 1.0, jax.random.fold_in(stream_key, 6)
    for dim, parts in shards:
        heights = jnp.exp(jax.random.uniform(jax.random.fold_in(own, dim), (parts,), jnp.float32, least / len(shards), top_value / len(shards)))
        loudness = loudness * jnp.repeat(heights, extent[dim] // parts).reshape([-1 if axis == dim else 1 for axis in range(len(extent))])
    return loudness


def deal_out(own_key, own, number, rows, number_of, top, reach, slope):
    sequence = jax.random.permutation(own_key, number_of)
    packed, common = portions_of(number_of, rows * top, reach, slope, True), portions_of(number_of, rows * top, reach, slope, False)
    places = jnp.arange(number_of)

    def named(lengths, turn):
        used = int((lengths > 0).sum())
        fixed = max(1, used // 4)
        passed = fixed + (places - fixed + turn * (used - fixed)) % max(1, number_of - fixed)
        return jnp.zeros((number_of,), jnp.int32).at[sequence[jnp.where(places < fixed, places, passed)]].set(jnp.asarray(lengths, jnp.int32))

    lengths = jnp.where(number % 4 == 0, named(packed, number // 4), named(common, number - number // 4 - 1))
    mixed = jax.random.permutation(jax.random.fold_in(own, 3), number_of)
    donor, receiver = mixed[0:number_of // 2 * 2:2], mixed[1:number_of // 2 * 2:2]
    slack = jnp.minimum(lengths[donor] - 1, reach - lengths[receiver]) // 2
    slack = jnp.where((donor == sequence[0]) | (receiver == sequence[0]) | (lengths[receiver] == 0), 0, jnp.maximum(slack, 0))
    passed = jax.random.randint(jax.random.fold_in(own, 4), (number_of // 2,), 0, 1 << 20) % (slack + 1)
    lengths = lengths.at[donor].add(-passed).at[receiver].add(passed)
    members = jnp.searchsorted(jnp.cumsum(lengths), jnp.arange(rows * top), side="right").astype(jnp.int32)
    grid = members.reshape(top, rows).T
    grid = grid[jax.random.permutation(jax.random.fold_in(own, 1), rows)]
    turn = jax.random.randint(jax.random.fold_in(own, 2), (rows, 1), 0, top)
    return jnp.take_along_axis(grid, (jnp.arange(top)[None, :] + turn) % top, axis=1)


def portions_of(count, total, limit, slope, full):
    portions = [(1 << 20) // math.isqrt(rank ** slope) + 1 for rank in range(1, count + 1)]
    largest = limit if full else min(limit, max(-(-total // count), total * portions[0] // sum(portions)))
    least = 1 if total - largest >= count - 1 else 0
    counts, rest = [largest] + [least] * (count - 1), total - largest - least * (count - 1)
    while rest > 0:
        candidates = [i for i in range(1, count) if counts[i] < largest] or [i for i in range(1, count) if counts[i] < limit]
        mass, budget = sum([portions[i] for i in candidates]), rest
        for i in candidates:
            more = min(limit - counts[i], max(1, budget * portions[i] // mass), rest)
            counts[i] = counts[i] + more
            rest = rest - more
    return np.array(counts)


def scatter_about(rng, dims, scale, limit, cuts=(), held_as=jnp.bfloat16):
    values = jax.random.normal(rng, dims, jnp.float32) * scale
    if len(cuts) > 0:
        values = shard_levels(rng, dims, cuts, -0.22, 0.18) * values
    return jnp.clip(values, min=-limit, max=limit).astype(held_as)


def setup_inputs(seed: int = 0, part: int = 0) -> dict:
    keys = jax.random.split(jax.random.key(seed), 8)
    part_splits = jax.random.split(jax.random.fold_in(keys[7], part), 8)
    prompt = scatter_about(part_splits[0], (TOKENS, D), 1.0, 6.0, ((0, 8),))
    routes_keys = jax.random.split(jax.random.fold_in(part_splits[1], 1), TOKENS // TOK_DEV)
    routes_turns = jax.random.permutation(jax.random.fold_in(part_splits[1], 3), TOKENS // TOK_DEV)
    routes = jax.vmap(lambda own, number: deal_out(jax.random.fold_in(part_splits[1], 2), own, number, TOK_DEV, EXPERTS, TOP, CAP, 1))(routes_keys, routes_turns).reshape((TOKENS, TOP))
    route_weight = jnp.clip(jnp.exp(math.log(1.0) - 1.609438 * jax.random.uniform(part_splits[2], (TOKENS, TOP), jnp.float32) ** shard_levels(part_splits[2], (TOKENS, TOP), ((0, 8),), -0.2, 0.2)), 0.2, 1.0)
    norm_gain = jnp.clip(1.0 + 0.18 * jax.random.normal(keys[3], (D,), jnp.float32), 0.1, 1.9)
    gate_train = scatter_about(keys[4], (EXPERTS, D, FF), 0.055, 0.4, ((1, 8), (2, 2)), jnp.float32)
    up_train = scatter_about(keys[5], (EXPERTS, D, FF), 0.055, 0.4, ((1, 8), (2, 2)), jnp.float32)
    down_train = scatter_about(keys[6], (EXPERTS, FF, D), 0.01, 0.07, ((1, 8), (2, 2)), jnp.float32)
    return {"prompt": prompt, "routes": routes, "route_weight": route_weight, "norm_gain": norm_gain, "gate_train": gate_train, "up_train": up_train, "down_train": down_train}


LIMIT = 7.0
ALPHA = 1.702
EPS = 1e-06

def expert_apply(rows, gate_one, up_one, down_one):
    gate_pre = jnp.dot(rows, gate_one, preferred_element_type=jnp.float32)
    up_pre = jnp.dot(rows, up_one, preferred_element_type=jnp.float32)
    gate_pre = jnp.minimum(gate_pre, LIMIT)
    up_pre = jnp.clip(up_pre, -LIMIT, LIMIT)
    hidden = ((up_pre + 1.0) * gate_pre * jax.nn.sigmoid(ALPHA * gate_pre)).astype(jnp.bfloat16)
    width = hidden.shape[1] // N_TP
    total = jnp.zeros((rows.shape[0], down_one.shape[1]), jnp.float32)
    for block in range(N_TP):
        part = jnp.dot(hidden[:, block * width:(block + 1) * width], down_one[block * width:(block + 1) * width], preferred_element_type=jnp.float32).astype(jnp.bfloat16)
        part = lax.optimization_barrier(part)
        total = total + part.astype(jnp.float32)
    return total.astype(jnp.bfloat16)

def reference(prompt, routes, route_weight, norm_gain, gate_train, up_train, down_train):
    gate_serve = (norm_gain[None, :, None] * gate_train).astype(jnp.bfloat16)
    up_serve = (norm_gain[None, :, None] * up_train).astype(jnp.bfloat16)
    down_serve = down_train.astype(jnp.bfloat16)
    values = prompt.astype(jnp.float32)
    normed = (values * lax.rsqrt(lax.optimization_barrier(jnp.mean(values * values, axis=-1, keepdims=True)) + EPS)).astype(jnp.bfloat16)
    flat_expert = routes.reshape(-1).astype(jnp.int32)
    flat_weight = route_weight.reshape(-1)
    most = N_FS * CAP
    experts = gate_serve.shape[0]

    def one_expert(carry, expert):
        chosen = flat_expert == expert
        picks = jnp.nonzero(chosen, size=most, fill_value=0)[0].astype(jnp.int32)
        live = jnp.arange(most, dtype=jnp.int32) < jnp.sum(chosen.astype(jnp.int32))
        token = (picks // TOP).astype(jnp.int32)
        rows = normed[token]
        result = expert_apply(rows, gate_serve[expert], up_serve[expert], down_serve[expert])
        scale = jnp.where(live, flat_weight[picks], 0.0).astype(jnp.float32)
        carry = carry.at[token].add(result.astype(jnp.float32) * scale[:, None])
        return (carry, None)
    start = jnp.zeros(normed.shape, jnp.float32)
    total, unused = lax.scan(one_expert, start, jnp.arange(experts, dtype=jnp.int32))
    return (gate_serve, up_serve, down_serve, total.astype(jnp.bfloat16))
```

```python
import functools

import jax
import jax.numpy as jnp
from jax import lax
from jax.experimental import pallas as pl
from jax.experimental.pallas import tpu as pltpu
from jax.sharding import PartitionSpec as P

LIMIT = 7.0
ALPHA = 1.702
EPS = 1e-06
MESH = pl.DeviceIdType.MESH


def exchange(
    sizes,
    scale_in,
    tok_in,
    gate_in,
    up_in,
    down_in,
    scale,
    tok,
    gate,
    up,
    down,
    recv_w,
    send_w,
    recv_t,
    send_up,
    send_dn,
    send_pt,
    recv_s,
    send_s,
    local,
):
    G, F, T = sizes
    g, f, t = lax.axis_index("grp"), lax.axis_index("fs"), lax.axis_index("tp")
    barrier = pltpu.get_barrier_semaphore()
    for axis, here, count in (("fs", f, F), ("grp", g, G), ("tp", t, T)):
        for s in range(1, count):
            pl.semaphore_signal(
                barrier, inc=1, device_id={axis: lax.rem(here + s, count)}, device_id_type=MESH
            )
    pl.semaphore_wait(barrier, F + G + T - 3)

    def remote(src, dst, send, recv, **where):
        return pltpu.make_async_remote_copy(
            src_ref=src, dst_ref=dst, send_sem=send, recv_sem=recv, device_id=where,
            device_id_type=MESH,
        )

    mats = ((gate_in, gate), (up_in, up), (down_in, down))

    def rows_of(m, src, gg, tt):
        block = mats[m][0].shape[1]
        piece = block // G
        start = (tt * F + src) * block + gg * piece
        return mats[m][1].at[pl.ds(pl.multiple_of(start, piece), piece)]

    def sent_piece(m, expert):
        piece = mats[m][0].shape[1] // G
        return mats[m][0].at[expert, pl.ds(pl.multiple_of(g * piece, piece), piece)]

    def wait_piece(m, src, gg, tt):
        ref = rows_of(m, src, gg, tt)
        remote(ref, ref, send_w.at[m], recv_w.at[m, src, gg, tt], fs=lax.rem(f + 1, F)).wait_recv()

    def pass_on(m, src, gg, tt, **where):
        ref = rows_of(m, src, gg, tt)
        remote(ref, ref, send_w.at[m], recv_w.at[m, src, gg, tt], **where).start()

    rows = tok_in.shape[0]

    def block_of(src):
        return tok.at[pl.ds(pl.multiple_of(src * rows, rows), rows)]

    Z = F // 2
    z, core = f // 2, lax.rem(f, 2)
    partner = f + 1 - 2 * core

    own_scale = pltpu.make_async_copy(scale_in.at[f], scale.at[f], local.at[4])
    own_scale.start()

    def scale_copy(to, src):
        return remote(scale_in.at[to], scale.at[src], send_s.at[to], recv_s.at[src], fs=to)

    own = [pltpu.make_async_copy(tok_in, block_of(f), local.at[3])]
    for m in range(3):
        own.append(pltpu.make_async_copy(sent_piece(m, f), rows_of(m, f, g, t), local.at[m]))
    for copy in own:
        copy.start()

    @pl.loop(1, F)
    def _(s):
        scale_copy(lax.rem(f + s, F), f).start()

    for m in range(3):

        @pl.loop(1, F)
        def _(s, m=m):
            to = lax.rem(f + s, F)
            remote(
                sent_piece(m, to), rows_of(m, f, g, t), send_w.at[m], recv_w.at[m, f, g, t], fs=to
            ).start()

    def tok_copy(src_ref, src, kind):
        sems, to = ((send_up, f + 2), (send_dn, f - 2), (send_pt, partner))[kind]
        return remote(src_ref, block_of(src), sems.at[src], recv_t.at[src], fs=to)

    @pl.when(z < Z - 1)
    def _():
        tok_copy(tok_in, f, 0).start()

    @pl.when(z > 0)
    def _():
        tok_copy(tok_in, f, 1).start()

    tok_copy(tok_in, f, 2).start()

    def first(m, src):
        for dg in range(1, G):
            pass_on(m, src, g, t, grp=lax.rem(g + dg, G))
        for dt in range(1, T):
            pass_on(m, src, g, t, tp=lax.rem(t + dt, T))

    def phase1(m):
        own[m + 1].wait()
        first(m, f)

        @pl.loop(1, F)
        def _(s):
            src = lax.rem(f - s + F, F)
            wait_piece(m, src, g, t)
            first(m, src)

    def phase2(m):
        @pl.loop(0, F)
        def _(s):
            src = lax.rem(f - s + F, F)
            even = lax.rem(src, 2) == 0
            for dg in range(1, G):
                gg = lax.rem(g + dg, G)
                wait_piece(m, src, gg, t)

                @pl.when(even)
                def _():
                    for dt in range(1, T):
                        pass_on(m, src, gg, t, tp=lax.rem(t + dt, T))

            for dt in range(1, T):
                tt = lax.rem(t + dt, T)
                wait_piece(m, src, g, tt)

                @pl.when(jnp.logical_not(even))
                def _():
                    for dg in range(1, G):
                        pass_on(m, src, g, tt, grp=lax.rem(g + dg, G))

    def chain(low, high):
        @pl.loop(low, high)
        def _(d):
            @pl.when(z >= d)
            def _():
                src = f - 2 * d
                tok_copy(block_of(src), src, 2).wait_recv()

                @pl.when(z < Z - 1)
                def _():
                    tok_copy(block_of(src), src, 0).start()

                tok_copy(block_of(src), src, 2).start()

            @pl.when(z + d < Z)
            def _():
                src = f + 2 * d
                tok_copy(block_of(src), src, 2).wait_recv()

                @pl.when(z > 0)
                def _():
                    tok_copy(block_of(src), src, 1).start()

                tok_copy(block_of(src), src, 2).start()

    phase1(0)
    phase1(1)
    phase2(0)
    phase1(2)
    chain(1, 2)
    phase2(1)
    chain(2, 3)
    phase2(2)
    chain(3, Z)

    for m in range(3):

        @pl.loop(0, F)
        def _(src, m=m):
            for dg in range(1, G):
                for dt in range(1, T):
                    wait_piece(m, src, lax.rem(g + dg, G), lax.rem(t + dt, T))

        out = mats[m][1]
        sent = out.at[pl.ds(0, out.shape[0] - mats[m][0].shape[1] // G)]
        remote(sent, sent, send_w.at[m], recv_w.at[m, 0, 0, 0], fs=lax.rem(f + 1, F)).wait_send()

    own[0].wait()
    own_scale.wait()

    @pl.loop(1, F)
    def _(s):
        to = lax.rem(f + s, F)
        scale_copy(to, to).wait_recv()
        scale_copy(to, f).wait_send()

    @pl.loop(0, Z)
    def _(zz):
        src = 2 * zz + core
        other = 2 * zz + 1 - core
        tok_copy(block_of(other), other, 2).wait_recv()
        tok_copy(block_of(src), src, 2).wait_send()

        @pl.when(jnp.logical_and(zz <= z, z < Z - 1))
        def _():
            tok_copy(block_of(src), src, 0).wait_send()

        @pl.when(jnp.logical_and(zz >= z, z > 0))
        def _():
            tok_copy(block_of(src), src, 1).wait_send()


def gathered(mesh, scale_in, tok_in, gate_in, up_in, down_in):
    G, F, T = (mesh.shape[name] for name in ("grp", "fs", "tp"))
    full = [
        jax.ShapeDtypeStruct((T * F * w.shape[1], w.shape[2]), w.dtype)
        for w in (gate_in, up_in, down_in)
    ]
    return pl.pallas_call(
        functools.partial(exchange, (G, F, T)),
        out_shape=[jax.ShapeDtypeStruct(scale_in.shape, scale_in.dtype)]
        + [jax.ShapeDtypeStruct((F * tok_in.shape[0], tok_in.shape[1]), tok_in.dtype)]
        + full,
        in_specs=[pl.BlockSpec(memory_space=pl.ANY)] * 5,
        out_specs=[pl.BlockSpec(memory_space=pltpu.VMEM)] * 5,
        scratch_shapes=[
            pltpu.SemaphoreType.DMA((3, F, G, T)),
            pltpu.SemaphoreType.DMA((3,)),
            pltpu.SemaphoreType.DMA((F,)),
            pltpu.SemaphoreType.DMA((F,)),
            pltpu.SemaphoreType.DMA((F,)),
            pltpu.SemaphoreType.DMA((F,)),
            pltpu.SemaphoreType.DMA((F,)),
            pltpu.SemaphoreType.DMA((F,)),
            pltpu.SemaphoreType.DMA((5,)),
        ],
        compiler_params=pltpu.CompilerParams(
            collective_id=0, has_side_effects=True, vmem_limit_bytes=40 * 1024 * 1024
        ),
    )(scale_in, tok_in, gate_in, up_in, down_in)


def chunk_rows(rows):
    return 48 if rows % 48 == 0 else rows


def combine(
    sizes,
    hidden,
    down,
    scale,
    out,
    comb,
    got,
    up_in,
    dn_in,
    pair_s,
    pair_r,
    up_s,
    up_r,
    dn_s,
    dn_r,
    x_s,
    x_r,
):
    G, F, T = sizes
    f, t = lax.axis_index("fs"), lax.axis_index("tp")
    Z = F // 2
    z, core = f // 2, lax.rem(f, 2)
    partner = f + 1 - 2 * core
    lower, upper = z > 0, z < Z - 1
    part, width = got.shape[1], got.shape[2]
    own = width // T
    rows = chunk_rows(part)
    chunks = part // rows
    inner = hidden.shape[1]
    tile = min(512, own)

    barrier = pltpu.get_barrier_semaphore()

    def greet(**where):
        pl.semaphore_signal(barrier, inc=1, device_id=where, device_id_type=MESH)

    greet(fs=partner)
    for dt in range(1, T):
        greet(tp=lax.rem(t + dt, T))
    pl.when(lower)(lambda: greet(fs=f - 2))
    pl.when(upper)(lambda: greet(fs=f + 2))
    pl.semaphore_wait(barrier, T + lower.astype(jnp.int32) + upper.astype(jnp.int32))

    def remote(src, dst, send, recv, **where):
        return pltpu.make_async_remote_copy(
            src_ref=src, dst_ref=dst, send_sem=send, recv_sem=recv, device_id=where,
            device_id_type=MESH,
        )

    def strip(q):
        return pl.ds(pl.multiple_of(q * rows, rows), rows)

    def pair_copy(d):
        return remote(comb.at[d, 1 - core], got.at[d], pair_s.at[d], pair_r.at[d], fs=partner)

    def up_copy(d, q):
        return remote(
            comb.at[d, core, strip(q)], up_in.at[d, strip(q)], up_s.at[d, q], up_r.at[d, q],
            fs=f + 2,
        )

    def dn_copy(d, q):
        return remote(
            comb.at[d, core, strip(q)], dn_in.at[d, strip(q)], dn_s.at[d, q], dn_r.at[d, q],
            fs=f - 2,
        )

    def x_copy(q, tt, src):
        start = pl.multiple_of(src * part + q * rows, rows)
        return remote(
            comb.at[z, core, strip(q), pl.ds(pl.multiple_of(tt * own, own), own)],
            out.at[pl.ds(start, rows)], x_s.at[q, tt], x_r.at[q, src], tp=tt,
        )

    def dest_of(k):
        half = k // 2
        d = jnp.where(lax.rem(k, 2) == 0, Z - 1 - half, half)
        return jnp.where(2 * z < Z, d, Z - 1 - d)

    def add(d, q, extra):
        here = comb[d, core, strip(q)].astype(jnp.float32)
        comb[d, core, strip(q)] = (here + extra[d, strip(q)].astype(jnp.float32)).astype(comb.dtype)

    def compute(d):
        tokens = pl.ds(pl.multiple_of(d * 2 * part, 2 * part), 2 * part)

        @pl.loop(0, width // tile)
        def _(i):
            tt, col = i // (own // tile), lax.rem(i, own // tile) * tile
            weights = down[
                pl.ds(pl.multiple_of(tt * inner, inner), inner),
                pl.ds(pl.multiple_of(col, tile), tile),
            ]
            value = jnp.dot(hidden[tokens], weights, preferred_element_type=jnp.float32)
            value = (value * scale[tokens]).astype(comb.dtype)
            comb[d, :, :, pl.ds(pl.multiple_of(i * tile, tile), tile)] = value.reshape(
                2, part, tile
            )

        pair_copy(d).start()

    def paired(d):
        pair_copy(d).wait_recv()

        @pl.loop(0, chunks)
        def _(q):
            add(d, q, got)

            @pl.when(jnp.logical_and(z == 0, d > z))
            def _():
                up_copy(d, q).start()

            @pl.when(jnp.logical_and(z == Z - 1, d < z))
            def _():
                dn_copy(d, q).start()

    compute(dest_of(0))

    @pl.loop(1, Z)
    def _(k):
        compute(dest_of(k))
        paired(dest_of(k - 1))

    paired(dest_of(Z - 1))

    ups, downs = 2 * z, 2 * (Z - 1 - z)
    last = jnp.maximum(
        jnp.where(lower, (Z - 1 - z) * chunks + ups, 0), jnp.where(upper, z * chunks + downs, 0)
    )

    @pl.loop(0, Z * chunks + 2 * Z)
    def _(step):
        u, v, w = step - ups, step - downs, step - last
        uq, vq = lax.rem(jnp.maximum(u, 0), chunks), lax.rem(jnp.maximum(v, 0), chunks)
        high, low = Z - 1 - jnp.maximum(u, 0) // chunks, jnp.maximum(v, 0) // chunks

        @pl.when(jnp.logical_and(jnp.logical_and(lower, u >= 0), high >= z))
        def _():
            up_copy(high, uq).wait_recv()
            add(high, uq, up_in)

            @pl.when(high > z)
            def _():
                up_copy(high, uq).start()

        @pl.when(jnp.logical_and(jnp.logical_and(upper, v >= 0), low <= z))
        def _():
            dn_copy(low, vq).wait_recv()
            add(low, vq, dn_in)

            @pl.when(low < z)
            def _():
                dn_copy(low, vq).start()

        @pl.when(jnp.logical_and(w >= 0, w < chunks))
        def _():
            for dt in range(1, T):
                x_copy(w, lax.rem(t + dt, T), t).start()
            start = pl.multiple_of(t * part + w * rows, rows)
            out[pl.ds(start, rows)] = comb[
                z, core, strip(w), pl.ds(pl.multiple_of(t * own, own), own)
            ]

    @pl.loop(0, Z)
    def _(d):
        pair_copy(d).wait_send()

        @pl.loop(0, chunks)
        def _(q):
            @pl.when(jnp.logical_and(upper, d > z))
            def _():
                up_copy(d, q).wait_send()

            @pl.when(jnp.logical_and(lower, d < z))
            def _():
                dn_copy(d, q).wait_send()

    @pl.loop(0, chunks)
    def _(q):
        for dt in range(1, T):
            tt = lax.rem(t + dt, T)
            x_copy(q, tt, t).wait_send()
            x_copy(q, tt, tt).wait_recv()


def combined(mesh, hidden, down, scale):
    G, F, T = (mesh.shape[name] for name in ("grp", "fs", "tp"))
    Z, part, width = F // 2, hidden.shape[0] // F, down.shape[1] * T
    chunks = part // chunk_rows(part)
    block = pltpu.VMEM((Z, part, width), hidden.dtype)
    pair, flow, cross = (
        pltpu.SemaphoreType.DMA((Z,)),
        pltpu.SemaphoreType.DMA((Z, chunks)),
        pltpu.SemaphoreType.DMA((chunks, T)),
    )
    return pl.pallas_call(
        functools.partial(combine, (G, F, T)),
        out_shape=jax.ShapeDtypeStruct((T * part, width // T), hidden.dtype),
        in_specs=[pl.BlockSpec(memory_space=pltpu.VMEM)] * 3,
        out_specs=pl.BlockSpec(memory_space=pltpu.VMEM),
        scratch_shapes=[pltpu.VMEM((Z, 2, part, width), hidden.dtype), block, block, block]
        + [pair, pair, flow, flow, flow, flow, cross, cross],
        compiler_params=pltpu.CompilerParams(
            collective_id=1, has_side_effects=True, vmem_limit_bytes=60 * 1024 * 1024
        ),
    )(hidden, down, scale)


def shards(mesh, prompt, routes, route_weight, norm_gain, gate_train, up_train, down_train):
    T = mesh.shape["tp"]
    t = lax.axis_index("tp")
    experts = gate_train.shape[0]
    tok_rows, width = prompt.shape
    part = tok_rows // T
    values = lax.dynamic_slice_in_dim(prompt, t * part, part, 0).astype(jnp.float32)
    normed = (values * lax.rsqrt(jnp.mean(values * values, axis=-1, keepdims=True) + EPS)).astype(
        jnp.bfloat16
    )
    lanes = jnp.arange(experts, dtype=jnp.int32)
    routes = lax.dynamic_slice_in_dim(routes, t * part, part, 0)
    route_weight = lax.dynamic_slice_in_dim(route_weight, t * part, part, 0)
    scale = jnp.sum(
        jnp.where(routes[:, :, None] == lanes[None, None, :], route_weight[:, :, None], 0.0), axis=1
    )

    gain = norm_gain[None, :, None]
    scale, tokens, gate, up, down = gathered(
        mesh,
        scale.T.reshape(experts, 1, part),
        normed,
        (gain * gate_train).astype(jnp.bfloat16),
        (gain * up_train).astype(jnp.bfloat16),
        down_train.astype(jnp.bfloat16),
    )
    scale = scale.reshape(-1, 1)
    gate, up, down = (w.reshape(T, w.shape[0] // T, w.shape[1]) for w in (gate, up, down))
    own = gate.shape[2]
    gate_mine = lax.dynamic_slice_in_dim(gate, t, 1, 0)
    up_mine = lax.dynamic_slice_in_dim(up, t, 1, 0)
    down_mine = lax.dynamic_slice_in_dim(down, t * own, own, 1)
    down_mine = down_mine.transpose(1, 0, 2).reshape(1, own, -1)

    hidden = []
    for i in range(T):
        gate_pre = jnp.dot(tokens, gate[i], preferred_element_type=jnp.float32)
        up_pre = jnp.dot(tokens, up[i], preferred_element_type=jnp.float32)
        gate_pre = jnp.minimum(gate_pre, LIMIT)
        up_pre = jnp.clip(up_pre, -LIMIT, LIMIT)
        hidden.append(
            ((up_pre + 1.0) * gate_pre * jax.nn.sigmoid(ALPHA * gate_pre)).astype(jnp.bfloat16)
        )
    hidden = jnp.concatenate(hidden, axis=1)
    mixed = combined(mesh, hidden, down.reshape(-1, down.shape[2]), scale)
    return (gate_mine, up_mine, down_mine, mixed)


def solution(mesh):
    return jax.shard_map(
        functools.partial(shards, mesh),
        mesh=mesh,
        in_specs=(
            P(("grp", "fs"), None),
            P(("grp", "fs"), None),
            P(("grp", "fs"), None),
            P("fs"),
            P(None, "fs", "tp"),
            P(None, "fs", "tp"),
            P(None, "fs", "tp"),
        ),
        out_specs=(
            P(("grp", "fs"), None, "tp"),
            P(("grp", "fs"), None, "tp"),
            P(("grp", "fs"), "tp", None),
            P(("grp", "fs"), "tp"),
        ),
        check_vma=False,
    )
```

```python
import functools

import jax
import jax.numpy as jnp
from jax import lax
from jax.experimental import pallas as pl
from jax.experimental.pallas import tpu as pltpu
from jax.sharding import PartitionSpec as P

LIMIT = 7.0
ALPHA = 1.702
EPS = 1e-06
MESH = pl.DeviceIdType.MESH


def chunk_rows(rows):
    return 48 if rows % 48 == 0 else rows


def layer(
    sizes,
    scale_in,
    tok_in,
    gate_in,
    up_in,
    down_in,
    gate,
    up,
    down,
    out,
    tok,
    hidden,
    comb,
    got,
    above,
    scale,
    weight,
    recv_w,
    send_w,
    recv_t,
    send_up,
    send_dn,
    send_pt,
    recv_s,
    send_s,
    local,
    pair_s,
    pair_r,
    up_s,
    up_r,
    dn_s,
    dn_r,
    x_s,
    x_r,
):
    G, F, T = sizes
    g, f, t = lax.axis_index("grp"), lax.axis_index("fs"), lax.axis_index("tp")
    Z = F // 2
    z, core = f // 2, lax.rem(f, 2)
    partner = f + 1 - 2 * core
    lower, upper = z > 0, z < Z - 1
    part, width = got.shape[1], got.shape[2]
    own = width // T
    rows = chunk_rows(part)
    chunks = part // rows
    inner = hidden.shape[1]
    tile = min(512, own)
    cols = gate.shape[1]
    strips = min(256, cols)
    tiles = inner // strips
    far = F - 2
    lag = far // 2

    barrier = pltpu.get_barrier_semaphore()
    for axis, here, count in (("fs", f, F), ("grp", g, G), ("tp", t, T)):
        for s in range(1, count):
            pl.semaphore_signal(
                barrier, inc=1, device_id={axis: lax.rem(here + s, count)}, device_id_type=MESH
            )
    pl.semaphore_wait(barrier, F + G + T - 3)

    def remote(src, dst, send, recv, **where):
        return pltpu.make_async_remote_copy(
            src_ref=src, dst_ref=dst, send_sem=send, recv_sem=recv, device_id=where,
            device_id_type=MESH,
        )

    mats = ((gate_in, gate), (up_in, up), (down_in, down))

    def block_rows(m, src, tt):
        block = mats[m][0].shape[1]
        return mats[m][1].at[pl.ds(pl.multiple_of((tt * F + src) * block, block), block)]

    def piece_rows(m, src, gg, tt):
        block = mats[m][0].shape[1]
        piece = block // G
        start = (tt * F + src) * block + gg * piece
        return mats[m][1].at[pl.ds(pl.multiple_of(start, piece), piece)]

    def sent_piece(m, expert):
        piece = mats[m][0].shape[1] // G
        return mats[m][0].at[expert, pl.ds(pl.multiple_of(g * piece, piece), piece)]

    def wait_piece(m, src, gg, tt):
        ref = piece_rows(m, src, gg, tt)
        remote(ref, ref, send_w.at[m], recv_w.at[m, src, gg, tt], fs=partner).wait_recv()

    def pass_piece(m, src, gg, tt, **where):
        ref = piece_rows(m, src, gg, tt)
        remote(ref, ref, send_w.at[m], recv_w.at[m, src, gg, tt], **where).start()

    def wait_block(m, src, tt):
        ref = block_rows(m, src, tt)
        remote(ref, ref, send_w.at[m], recv_w.at[m, src, 0, tt], fs=partner).wait_recv()

    def near_blocks(m, src_ref, src):
        for dt in range(1, T):
            remote(
                src_ref, block_rows(m, src, t), send_w.at[m], recv_w.at[m, src, 0, t],
                tp=lax.rem(t + dt, T),
            ).start()

    def far_source(r):
        return lax.rem(f - (r + 1 + core) + F, F)

    def own_block(m):
        return pltpu.make_async_copy(mats[m][0].at[f], block_rows(m, f, t), local.at[m])

    def token_block(src):
        return tok.at[pl.ds(pl.multiple_of(src * part, part), part)]

    def token_rows(src, q):
        return tok.at[pl.ds(pl.multiple_of(src * part + q * rows, rows), rows)]

    own_tokens = pltpu.make_async_copy(tok_in, token_block(f), local.at[3])
    own_scale = pltpu.make_async_copy(scale_in.at[f], scale.at[f], local.at[4])

    def scale_copy(to, src):
        return remote(scale_in.at[to], scale.at[src], send_s.at[to], recv_s.at[src], fs=to)

    def token_copy(src_ref, src, q, kind):
        sems, to = ((send_up, f + 2), (send_dn, f - 2), (send_pt, partner))[kind]
        return remote(src_ref, token_rows(src, q), sems.at[src, q], recv_t.at[src, q], fs=to)

    own_scale.start()
    own_tokens.start()
    for m in range(3):
        own_block(m).start()
        remote(
            mats[m][0].at[partner], block_rows(m, f, t), send_w.at[m], recv_w.at[m, f, 0, t],
            fs=partner,
        ).start()

    @pl.loop(1, F)
    def _(s):
        scale_copy(lax.rem(f + s, F), f).start()

    near_blocks(0, mats[0][0].at[f], f)
    for m in range(3):

        @pl.loop(0, far)
        def _(r, m=m):
            to = lax.rem(f + r + 2 - core, F)
            remote(
                sent_piece(m, to), piece_rows(m, f, g, t), send_w.at[m], recv_w.at[m, f, g, t],
                fs=to,
            ).start()

    @pl.loop(0, chunks)
    def _(q):
        source = tok_in.at[pl.ds(pl.multiple_of(q * rows, rows), rows)]

        @pl.when(upper)
        def _():
            token_copy(source, f, q, 0).start()

        @pl.when(lower)
        def _():
            token_copy(source, f, q, 1).start()

        token_copy(source, f, q, 2).start()

    def first(m, r):
        src = far_source(r)
        wait_piece(m, src, g, t)
        for dg in range(1, G):
            pass_piece(m, src, g, t, grp=lax.rem(g + dg, G))
        for dt in range(1, T):
            pass_piece(m, src, g, t, tp=lax.rem(t + dt, T))

    def second(m, r):
        src = far_source(r)
        across = lax.rem(r, 6) == 0
        for dg in range(1, G):
            gg = lax.rem(g + dg, G)
            wait_piece(m, src, gg, t)

            @pl.when(across)
            def _():
                for dt in range(1, T):
                    pass_piece(m, src, gg, t, tp=lax.rem(t + dt, T))

        for dt in range(1, T):
            tt = lax.rem(t + dt, T)
            wait_piece(m, src, g, tt)

            @pl.when(jnp.logical_not(across))
            def _():
                for dg in range(1, G):
                    pass_piece(m, src, g, tt, grp=lax.rem(g + dg, G))

    def settle(m):
        own_block(m).wait()

        @pl.loop(0, far)
        def _(r):
            for dg in range(1, G):
                for dt in range(1, T):
                    wait_piece(m, far_source(r), lax.rem(g + dg, G), lax.rem(t + dt, T))

        for src in (f, partner):
            for dt in range(1, T):
                wait_block(m, src, lax.rem(t + dt, T))

    for m in range(3):
        if m > 0:
            near_blocks(m, mats[m][0].at[f], f)
        wait_block(m, partner, t)
        near_blocks(m, block_rows(m, partner, t), partner)

        @pl.loop(0, far)
        def _(r, m=m):
            first(m, r)

            @pl.when(r >= lag)
            def _():
                second(m, r - lag)

            if m > 0:

                @pl.when(r < lag)
                def _():
                    second(m - 1, far - lag + r)

    def chain(d, q):
        @pl.when(z >= d)
        def _():
            src = f - 2 * d
            token_copy(token_rows(src, q), src, q, 2).wait_recv()

            @pl.when(upper)
            def _():
                token_copy(token_rows(src, q), src, q, 0).start()

            token_copy(token_rows(src, q), src, q, 2).start()

        @pl.when(z + d < Z)
        def _():
            src = f + 2 * d
            token_copy(token_rows(src, q), src, q, 2).wait_recv()

            @pl.when(lower)
            def _():
                token_copy(token_rows(src, q), src, q, 1).start()

            token_copy(token_rows(src, q), src, q, 2).start()

    def tokens_of(d):
        return pl.ds(pl.multiple_of(d * 2 * part, 2 * part), 2 * part)

    def partner_tokens(d):
        src = 2 * d + 1 - core

        @pl.loop(0, chunks)
        def _(q):
            token_copy(token_rows(src, q), src, q, 2).wait_recv()

    def hidden_tile(d, i):
        per = cols // strips
        tt, col = i // per, lax.rem(i, per) * strips
        where = (
            pl.ds(pl.multiple_of(tt * width, width), width),
            pl.ds(pl.multiple_of(col, strips), strips),
        )
        held = tok[tokens_of(d)]
        gate_pre = jnp.dot(held, gate[where], preferred_element_type=jnp.float32)
        up_pre = jnp.dot(held, up[where], preferred_element_type=jnp.float32)
        gate_pre = jnp.minimum(gate_pre, LIMIT)
        up_pre = jnp.clip(up_pre, -LIMIT, LIMIT)
        value = (up_pre + 1.0) * gate_pre * jax.nn.sigmoid(ALPHA * gate_pre)
        hidden[tokens_of(d), pl.ds(pl.multiple_of(i * strips, strips), strips)] = value.astype(
            hidden.dtype
        )

    own_tokens.wait()
    settle(0)
    settle(1)

    @pl.loop(0, Z)
    def _(d):
        low, high = z - d, z + d
        pl.when(low >= 0)(lambda: partner_tokens(low))
        pl.when(jnp.logical_and(d > 0, high < Z))(lambda: partner_tokens(high))

        @pl.loop(0, chunks)
        def _(q):
            pl.when(d + 1 < Z)(lambda: chain(d + 1, q))

            @pl.when(d == 0)
            def _():
                @pl.loop(far - lag + q * lag // chunks, far - lag + (q + 1) * lag // chunks)
                def _(r):
                    second(2, r)

            @pl.loop(q * tiles // chunks, (q + 1) * tiles // chunks)
            def _(i):
                pl.when(low >= 0)(lambda: hidden_tile(low, i))
                pl.when(jnp.logical_and(d > 0, high < Z))(lambda: hidden_tile(high, i))

    own_scale.wait()

    @pl.loop(1, F)
    def _(s):
        to = lax.rem(f + s, F)
        scale_copy(to, to).wait_recv()

    @pl.loop(0, F)
    def _(src):
        row = lax.broadcasted_iota(jnp.int32, (part, part), 0)
        lane = lax.broadcasted_iota(jnp.int32, (part, part), 1)
        spread = jnp.where(row == lane, scale[src], 0.0)
        weight[pl.ds(pl.multiple_of(src * part, part), part)] = jnp.broadcast_to(
            jnp.sum(spread, axis=1, keepdims=True), (part, weight.shape[1])
        )

    settle(2)

    def strip(q):
        return pl.ds(pl.multiple_of(q * rows, rows), rows)

    def pair_copy(d):
        return remote(comb.at[d, 1 - core], got.at[d], pair_s.at[d], pair_r.at[d], fs=partner)

    def up_copy(d, q):
        return remote(
            comb.at[d, core, strip(q)], above.at[d, strip(q)], up_s.at[d, q], up_r.at[d, q],
            fs=f + 2,
        )

    def dn_copy(d, q):
        return remote(
            comb.at[d, core, strip(q)], above.at[jnp.where(d == z - 1, Z, d), strip(q)], dn_s.at[d, q],
            dn_r.at[d, q],
            fs=f - 2,
        )

    def x_copy(q, tt, src):
        start = pl.multiple_of(src * part + q * rows, rows)
        return remote(
            comb.at[z, core, strip(q), pl.ds(pl.multiple_of(tt * own, own), own)],
            out.at[pl.ds(start, rows)], x_s.at[q, tt], x_r.at[q, src], tp=tt,
        )

    def dest_of(k):
        half = k // 2
        d = jnp.where(lax.rem(k, 2) == 0, Z - 1 - half, half)
        return jnp.where(2 * z < Z, d, Z - 1 - d)

    def add(d, q, extra, e):
        here = comb[d, core, strip(q)].astype(jnp.float32)
        comb[d, core, strip(q)] = (here + extra[e, strip(q)].astype(jnp.float32)).astype(comb.dtype)

    def compute(d):
        tokens = tokens_of(d)
        factor = jnp.concatenate([weight[tokens]] * (tile // weight.shape[1]), axis=1)

        @pl.loop(0, width // tile)
        def _(i):
            tt, col = i // (own // tile), lax.rem(i, own // tile) * tile
            weights = down[
                pl.ds(pl.multiple_of(tt * inner, inner), inner),
                pl.ds(pl.multiple_of(col, tile), tile),
            ]
            value = jnp.dot(hidden[tokens], weights, preferred_element_type=jnp.float32)
            value = (value * factor).astype(comb.dtype)
            comb[d, :, :, pl.ds(pl.multiple_of(i * tile, tile), tile)] = value.reshape(
                2, part, tile
            )

        pair_copy(d).start()

    def paired(d):
        pair_copy(d).wait_recv()

        @pl.loop(0, chunks)
        def _(q):
            add(d, q, got, d)

            @pl.when(jnp.logical_and(z == 0, d > z))
            def _():
                up_copy(d, q).start()

            @pl.when(jnp.logical_and(z == Z - 1, d < z))
            def _():
                dn_copy(d, q).start()

    compute(dest_of(0))

    @pl.loop(1, Z)
    def _(k):
        compute(dest_of(k))
        paired(dest_of(k - 1))

    paired(dest_of(Z - 1))

    ups, downs = 2 * z, 2 * (Z - 1 - z)
    last = jnp.maximum(
        jnp.where(lower, (Z - 1 - z) * chunks + ups, 0), jnp.where(upper, z * chunks + downs, 0)
    )

    @pl.loop(0, Z * chunks + 2 * Z)
    def _(step):
        u, v, w = step - ups, step - downs, step - last
        uq, vq = lax.rem(jnp.maximum(u, 0), chunks), lax.rem(jnp.maximum(v, 0), chunks)
        high, low = Z - 1 - jnp.maximum(u, 0) // chunks, jnp.maximum(v, 0) // chunks

        @pl.when(jnp.logical_and(jnp.logical_and(lower, u >= 0), high >= z))
        def _():
            up_copy(high, uq).wait_recv()
            add(high, uq, above, high)

            @pl.when(high > z)
            def _():
                up_copy(high, uq).start()

        @pl.when(jnp.logical_and(jnp.logical_and(upper, v >= 0), low <= z))
        def _():
            dn_copy(low, vq).wait_recv()
            add(low, vq, above, jnp.where(low == z, Z, low))

            @pl.when(low < z)
            def _():
                dn_copy(low, vq).start()

        @pl.when(jnp.logical_and(w >= 0, w < chunks))
        def _():
            for dt in range(1, T):
                x_copy(w, lax.rem(t + dt, T), t).start()
            start = pl.multiple_of(t * part + w * rows, rows)
            out[pl.ds(start, rows)] = comb[
                z, core, strip(w), pl.ds(pl.multiple_of(t * own, own), own)
            ]

    @pl.loop(0, Z)
    def _(d):
        pair_copy(d).wait_send()

        @pl.loop(0, chunks)
        def _(q):
            @pl.when(jnp.logical_and(upper, d > z))
            def _():
                up_copy(d, q).wait_send()

            @pl.when(jnp.logical_and(lower, d < z))
            def _():
                dn_copy(d, q).wait_send()

    @pl.loop(0, chunks)
    def _(q):
        for dt in range(1, T):
            tt = lax.rem(t + dt, T)
            x_copy(q, tt, t).wait_send()
            x_copy(q, tt, tt).wait_recv()

    for m in range(3):
        sent = mats[m][1].at[pl.ds(0, mats[m][1].shape[0] - mats[m][0].shape[1])]
        remote(sent, sent, send_w.at[m], recv_w.at[m, 0, 0, 0], fs=partner).wait_send()

    @pl.loop(1, F)
    def _(s):
        scale_copy(lax.rem(f + s, F), f).wait_send()

    @pl.loop(0, Z)
    def _(d):
        src = 2 * d + core

        @pl.loop(0, chunks)
        def _(q):
            token_copy(token_rows(src, q), src, q, 2).wait_send()

            @pl.when(jnp.logical_and(d <= z, upper))
            def _():
                token_copy(token_rows(src, q), src, q, 0).wait_send()

            @pl.when(jnp.logical_and(d >= z, lower))
            def _():
                token_copy(token_rows(src, q), src, q, 1).wait_send()


def deliver(T, gate, up, down, mixed, gate_out, up_out, down_out, mixed_out, sems):
    t = lax.axis_index("tp")
    depth, own, width = gate_out.shape[1], down_out.shape[1], down.shape[1]
    deep = pl.ds(pl.multiple_of(t * depth, depth), depth)
    copies = [
        pltpu.make_async_copy(gate.at[deep], gate_out.at[0], sems.at[0]),
        pltpu.make_async_copy(up.at[deep], up_out.at[0], sems.at[1]),
        pltpu.make_async_copy(mixed, mixed_out, sems.at[2]),
    ]
    for tt in range(T):
        source = down.at[pl.ds(pl.multiple_of((tt * T + t) * own, own), own)]
        copies.append(
            pltpu.make_async_copy(
                source, down_out.at[0, :, pl.ds(tt * width, width)], sems.at[3 + tt]
            )
        )
    for copy in copies:
        copy.start()
    for copy in copies:
        copy.wait()


def shards(mesh, prompt, routes, route_weight, norm_gain, gate_train, up_train, down_train):
    G, F, T = (mesh.shape[name] for name in ("grp", "fs", "tp"))
    Z = F // 2
    t = lax.axis_index("tp")
    experts = gate_train.shape[0]
    tok_rows, width = prompt.shape
    part = tok_rows // T
    values = lax.dynamic_slice_in_dim(prompt, t * part, part, 0).astype(jnp.float32)
    normed = (values * lax.rsqrt(jnp.mean(values * values, axis=-1, keepdims=True) + EPS)).astype(
        jnp.bfloat16
    )
    lanes = jnp.arange(experts, dtype=jnp.int32)
    routes = lax.dynamic_slice_in_dim(routes, t * part, part, 0)
    route_weight = lax.dynamic_slice_in_dim(route_weight, t * part, part, 0)
    scale = jnp.sum(
        jnp.where(routes[:, :, None] == lanes[None, None, :], route_weight[:, :, None], 0.0), axis=1
    )

    gain = norm_gain[None, :, None]
    scale = scale.T.reshape(experts, 1, part)
    mats = (
        (gain * gate_train).astype(jnp.bfloat16),
        (gain * up_train).astype(jnp.bfloat16),
        down_train.astype(jnp.bfloat16),
    )
    full = [jax.ShapeDtypeStruct((T * F * w.shape[1], w.shape[2]), w.dtype) for w in mats]
    mixed = jax.ShapeDtypeStruct((tok_rows, width // T), normed.dtype)
    inner = T * mats[0].shape[2]
    chunks = part // chunk_rows(part)
    bf16, f32, dma = jnp.bfloat16, jnp.float32, pltpu.SemaphoreType.DMA
    scratch = 2 * F * part * (4 * width + inner + 256) + part * width * 2
    room = 2 * sum(w.size for w in full + [mixed]) + scratch + 4 * 1024 * 1024
    held = pl.pallas_call(
        functools.partial(layer, (G, F, T)),
        out_shape=full + [mixed],
        in_specs=[pl.BlockSpec(memory_space=pl.ANY)] * 5,
        out_specs=[pl.BlockSpec(memory_space=pltpu.VMEM)] * 4,
        scratch_shapes=[
            pltpu.VMEM((F * part, width), bf16),
            pltpu.VMEM((F * part, inner), bf16),
            pltpu.VMEM((Z, 2, part, width), bf16),
            pltpu.VMEM((Z, part, width), bf16),
            pltpu.VMEM((Z + 1, part, width), bf16),
            pltpu.VMEM((F, 1, part), f32),
            pltpu.VMEM((F * part, 128), f32),
            dma((3, F, G, T)),
            dma((3,)),
            dma((F, chunks)),
            dma((F, chunks)),
            dma((F, chunks)),
            dma((F, chunks)),
            dma((F,)),
            dma((F,)),
            dma((5,)),
            dma((Z,)),
            dma((Z,)),
            dma((Z, chunks)),
            dma((Z, chunks)),
            dma((Z, chunks)),
            dma((Z, chunks)),
            dma((chunks, T)),
            dma((chunks, T)),
        ],
        compiler_params=pltpu.CompilerParams(
            collective_id=0, has_side_effects=True, vmem_limit_bytes=min(room, 63 * 1024 * 1024)
        ),
    )(scale, normed, *mats)
    return pl.pallas_call(
        functools.partial(deliver, T),
        out_shape=[
            jax.ShapeDtypeStruct((1, full[0].shape[0] // T, full[0].shape[1]), bf16),
            jax.ShapeDtypeStruct((1, full[1].shape[0] // T, full[1].shape[1]), bf16),
            jax.ShapeDtypeStruct((1, inner // T, width), bf16),
            mixed,
        ],
        in_specs=[pl.BlockSpec(memory_space=pl.ANY)] * 4,
        out_specs=[pl.BlockSpec(memory_space=pl.ANY)] * 4,
        scratch_shapes=[dma((3 + T,))],
        compiler_params=pltpu.CompilerParams(vmem_limit_bytes=1024 * 1024),
    )(*held)


def solution(mesh):
    return jax.shard_map(
        functools.partial(shards, mesh),
        mesh=mesh,
        in_specs=(
            P(("grp", "fs"), None),
            P(("grp", "fs"), None),
            P(("grp", "fs"), None),
            P("fs"),
            P(None, "fs", "tp"),
            P(None, "fs", "tp"),
            P(None, "fs", "tp"),
        ),
        out_specs=(
            P(("grp", "fs"), None, "tp"),
            P(("grp", "fs"), None, "tp"),
            P(("grp", "fs"), "tp", None),
            P(("grp", "fs"), "tp"),
        ),
        check_vma=False,
    )
```

```python
import functools

import jax
import jax.numpy as jnp
from jax import lax
from jax.experimental import pallas as pl
from jax.experimental.pallas import tpu as pltpu
from jax.sharding import PartitionSpec as P

LIMIT = 7.0
ALPHA = 1.702
EPS = 1e-06
MESH = pl.DeviceIdType.MESH


def chunk_rows(rows):
    return 48 if rows % 48 == 0 else rows


def layer(
    sizes,
    scale_in,
    prompt,
    gain_in,
    gate_in,
    up_in,
    down_in,
    gate,
    up,
    down,
    out,
    tok,
    hidden,
    comb,
    pair,
    got,
    above,
    scale,
    weight,
    gain,
    ready_g,
    ready_u,
    ready_d,
    raw_g,
    raw_u,
    raw_d,
    raw_s,
    recv_w,
    send_w,
    recv_t,
    send_up,
    send_dn,
    send_pt,
    recv_s,
    send_s,
    local,
    pair_s,
    pair_r,
    up_s,
    up_r,
    dn_s,
    dn_r,
    x_s,
    x_r,
):
    G, F, T = sizes
    g, f, t = lax.axis_index("grp"), lax.axis_index("fs"), lax.axis_index("tp")
    Z = F // 2
    z, core = f // 2, lax.rem(f, 2)
    partner = f + 1 - 2 * core
    lower, upper = z > 0, z < Z - 1
    part, width = tok.shape[0] // F, tok.shape[1]
    own = width // T
    rows = chunk_rows(part)
    chunks = part // rows
    inner = hidden.shape[1]
    tile = got.shape[3]
    parts = width // tile
    per_own = own // tile
    cols = gate.shape[1]
    strips = min(256, cols)
    tiles = inner // strips
    far = F - 2
    lag = far // 2

    barrier = pltpu.get_barrier_semaphore()
    for axis, here, count in (("fs", f, F), ("grp", g, G), ("tp", t, T)):
        for s in range(1, count):
            pl.semaphore_signal(
                barrier, inc=1, device_id={axis: lax.rem(here + s, count)}, device_id_type=MESH
            )
    pl.semaphore_wait(barrier, F + G + T - 3)

    def remote(src, dst, send, recv, **where):
        return pltpu.make_async_remote_copy(
            src_ref=src, dst_ref=dst, send_sem=send, recv_sem=recv, device_id=where,
            device_id_type=MESH,
        )

    mats = ((ready_g, gate), (ready_u, up), (ready_d, down))
    trained = ((gate_in, raw_g), (up_in, raw_u), (down_in, raw_d))
    slots = raw_g.shape[0]

    def block_rows(m, src, tt):
        block = mats[m][0].shape[1]
        return mats[m][1].at[pl.ds(pl.multiple_of((tt * F + src) * block, block), block)]

    def piece_rows(m, src, gg, tt):
        block = mats[m][0].shape[1]
        piece = block // G
        start = (tt * F + src) * block + gg * piece
        return mats[m][1].at[pl.ds(pl.multiple_of(start, piece), piece)]

    def sent_piece(m, expert):
        piece = mats[m][0].shape[1] // G
        return mats[m][0].at[expert, pl.ds(pl.multiple_of(g * piece, piece), piece)]

    def wait_piece(m, src, gg, tt):
        ref = piece_rows(m, src, gg, tt)
        remote(ref, ref, send_w.at[m], recv_w.at[m, src, gg, tt], fs=partner).wait_recv()

    def pass_piece(m, src, gg, tt, **where):
        ref = piece_rows(m, src, gg, tt)
        remote(ref, ref, send_w.at[m], recv_w.at[m, src, gg, tt], **where).start()

    def wait_block(m, src, tt):
        ref = block_rows(m, src, tt)
        remote(ref, ref, send_w.at[m], recv_w.at[m, src, 0, tt], fs=partner).wait_recv()

    def near_blocks(m, src_ref, src):
        for dt in range(1, T):
            remote(
                src_ref, block_rows(m, src, t), send_w.at[m], recv_w.at[m, src, 0, t],
                tp=lax.rem(t + dt, T),
            ).start()

    both = jnp.minimum(z, Z - 1 - z)
    rising = jnp.where(2 * z < Z, 1, -1)

    def far_peer(r):
        k, side = r // 2, lax.rem(r, 2)
        near = (k // 2 + 1) * (2 * lax.rem(k, 2) - 1)
        chip = z + rising * jnp.where(k < 2 * both, near, k - both + 1)
        return 2 * chip + jnp.where(side == 0, core, 1 - core)

    def token_block(src):
        return tok.at[pl.ds(pl.multiple_of(src * part, part), part)]

    def token_rows(src, q):
        return tok.at[pl.ds(pl.multiple_of(src * part + q * rows, rows), rows)]

    own_tokens = pltpu.make_async_copy(
        prompt.at[pl.ds(pl.multiple_of(t * part, part), part)], token_block(f), local.at[0]
    )
    own_scale = pltpu.make_async_copy(scale_in.at[f], scale.at[f], local.at[1])

    def scale_copy(to, src):
        return remote(scale_in.at[to], scale.at[src], send_s.at[to], recv_s.at[src], fs=to)

    def token_copy(src_ref, src, q, kind):
        sems, to = ((send_up, f + 2), (send_dn, f - 2), (send_pt, partner))[kind]
        return remote(src_ref, token_rows(src, q), sems.at[src, q], recv_t.at[src, q], fs=to)

    def column(values):
        size = values.shape[1]
        row = lax.broadcasted_iota(jnp.int32, (size, size), 0)
        lane = lax.broadcasted_iota(jnp.int32, (size, size), 1)
        spread = jnp.where(row == lane, values, 0.0)
        return jnp.broadcast_to(jnp.sum(spread, axis=1, keepdims=True), (size, 128))

    def expert_of(i):
        return jnp.where(i == 0, partner, jnp.where(i == 1, f, far_peer(jnp.maximum(i - 2, 0))))

    def load(m, i):
        slot = lax.rem(i, slots)
        return pltpu.make_async_copy(
            trained[m][0].at[expert_of(i)], trained[m][1].at[slot], raw_s.at[m, slot]
        )

    for m in range(3):
        pl.loop(0, min(slots, F))(lambda i, m=m: load(m, i).start())

    def convert(m, i):
        load(m, i).wait()
        value = trained[m][1][lax.rem(i, slots)]
        if m < 2:
            value = value * jnp.concatenate([gain[...]] * (value.shape[1] // 128), axis=1)
        value = value.astype(mats[m][0].dtype)
        mats[m][0][expert_of(i)] = value
        block = value.shape[0]

        @pl.when(i == 1)
        def _():
            start = pl.multiple_of((t * F + f) * block, block)
            mats[m][1][pl.ds(start, block)] = value

        pl.when(i + slots < F)(lambda: load(m, i + slots).start())

    def send_piece(m, r):
        to = far_peer(r)
        remote(
            sent_piece(m, to), piece_rows(m, f, g, t), send_w.at[m], recv_w.at[m, f, g, t], fs=to
        ).start()

    def emit(m, i):
        @pl.when(i == 0)
        def _():
            remote(
                mats[m][0].at[partner], block_rows(m, f, t), send_w.at[m], recv_w.at[m, f, 0, t],
                fs=partner,
            ).start()

        if m == 0:
            pl.when(i == 1)(lambda: near_blocks(0, mats[0][0].at[f], f))
            pl.when(i > 1)(lambda: send_piece(m, i - 2))

    def send_tokens(q):
        source = token_rows(f, q)
        pl.when(upper)(lambda: token_copy(source, f, q, 0).start())
        pl.when(lower)(lambda: token_copy(source, f, q, 1).start())
        token_copy(source, f, q, 2).start()

    own_scale.start()
    own_tokens.start()

    @pl.loop(1, F)
    def _(s):
        scale_copy(lax.rem(f + s, F), f).start()

    gain[...] = column(gain_in[...])
    for m in range(3):

        @pl.loop(0, F + 1)
        def _(i, m=m):
            pl.when(i < F)(lambda: convert(m, i))
            pl.when(i > 0)(lambda: emit(m, i - 1))

    own_tokens.wait()

    @pl.loop(0, chunks)
    def _(q):
        where = pl.ds(pl.multiple_of(f * part + q * rows, rows), rows)
        values = tok[where].astype(jnp.float32)
        mean = jnp.mean(values * values, axis=-1, keepdims=True)
        tok[where] = (values * lax.rsqrt(mean + EPS)).astype(tok.dtype)

    def first(m, r):
        src = far_peer(r)
        wait_piece(m, src, g, t)
        for dg in range(1, G):
            pass_piece(m, src, g, t, grp=lax.rem(g + dg, G))
        for dt in range(1, T):
            pass_piece(m, src, g, t, tp=lax.rem(t + dt, T))

    def second(m, r):
        src = far_peer(r)
        across = lax.rem(r, 6) == 0
        for dg in range(1, G):
            gg = lax.rem(g + dg, G)
            wait_piece(m, src, gg, t)

            @pl.when(across)
            def _():
                for dt in range(1, T):
                    pass_piece(m, src, gg, t, tp=lax.rem(t + dt, T))

        for dt in range(1, T):
            tt = lax.rem(t + dt, T)
            wait_piece(m, src, g, tt)

            @pl.when(jnp.logical_not(across))
            def _():
                for dg in range(1, G):
                    pass_piece(m, src, g, tt, grp=lax.rem(g + dg, G))

    def settle(m):
        @pl.loop(0, far)
        def _(r):
            for dg in range(1, G):
                for dt in range(1, T):
                    wait_piece(m, far_peer(r), lax.rem(g + dg, G), lax.rem(t + dt, T))

        for src in (f, partner):
            for dt in range(1, T):
                wait_block(m, src, lax.rem(t + dt, T))

    def chain(d, q):
        @pl.when(z >= d)
        def _():
            src = f - 2 * d
            token_copy(token_rows(src, q), src, q, 2).wait_recv()

            @pl.when(upper)
            def _():
                token_copy(token_rows(src, q), src, q, 0).start()

            token_copy(token_rows(src, q), src, q, 2).start()

        @pl.when(z + d < Z)
        def _():
            src = f + 2 * d
            token_copy(token_rows(src, q), src, q, 2).wait_recv()

            @pl.when(lower)
            def _():
                token_copy(token_rows(src, q), src, q, 1).start()

            token_copy(token_rows(src, q), src, q, 2).start()

    def tokens_of(d):
        return pl.ds(pl.multiple_of(d * 2 * part, 2 * part), 2 * part)

    def partner_tokens(d):
        src = 2 * d + 1 - core

        @pl.loop(0, chunks)
        def _(q):
            token_copy(token_rows(src, q), src, q, 2).wait_recv()

    def hidden_tile(d, i):
        per = cols // strips
        tt, col = i // per, lax.rem(i, per) * strips
        where = (
            pl.ds(pl.multiple_of(tt * width, width), width),
            pl.ds(pl.multiple_of(col, strips), strips),
        )
        held = tok[tokens_of(d)]
        gate_pre = jnp.dot(held, gate[where], preferred_element_type=jnp.float32)
        up_pre = jnp.dot(held, up[where], preferred_element_type=jnp.float32)
        gate_pre = jnp.minimum(gate_pre, LIMIT)
        up_pre = jnp.clip(up_pre, -LIMIT, LIMIT)
        value = (up_pre + 1.0) * gate_pre * jax.nn.sigmoid(ALPHA * gate_pre)
        hidden[tokens_of(d), pl.ds(pl.multiple_of(i * strips, strips), strips)] = value.astype(
            hidden.dtype
        )

    def span(i, count, total):
        return pl.loop(i * total // count, (i + 1) * total // count)

    for m in range(3):
        if m > 0:
            near_blocks(m, mats[m][0].at[f], f)
        if m == 2:
            pl.loop(far - lag, far)(lambda r: second(1, r))
            pl.loop(0, chunks)(lambda q: chain(1, q))

        @pl.loop(0, far)
        def _(r, m=m):
            first(m, r)
            if m == 0:
                send_piece(1, r)

            @pl.when(r >= lag)
            def _():
                second(m, r - lag)

            if m == 1:

                @pl.when(r < lag)
                def _():
                    second(m - 1, far - lag + r)

            if m == 1:

                @pl.when(r < lag)
                def _():
                    span(r, lag, chunks)(send_tokens)

                @pl.when(r >= lag)
                def _():
                    span(r - lag, far - lag, far)(lambda k: send_piece(2, k))

            if m == 2:

                @pl.when(r == lag)
                def _():
                    partner_tokens(z)
                    settle(0)
                    settle(1)

                @pl.when(r >= lag)
                def _():
                    span(r - lag, far - lag, tiles)(lambda i: hidden_tile(z, i))

        wait_block(m, partner, t)
        near_blocks(m, block_rows(m, partner, t), partner)

    def pair_copy(d, q, slot):
        return remote(
            pair.at[slot, 1 - core], got.at[d, q], pair_s.at[slot], pair_r.at[d, q], fs=partner
        )

    def up_copy(d, q):
        return remote(
            comb.at[d, q], above.at[d, q], up_s.at[d, q], up_r.at[d, q], fs=f + 2
        )

    def dn_copy(d, q):
        return remote(
            comb.at[d, q], above.at[jnp.where(d == z - 1, Z, d), q], dn_s.at[d, q],
            dn_r.at[d, q], fs=f - 2,
        )

    def home(src, q):
        return (
            pl.ds(pl.multiple_of(src * part, part), part),
            pl.ds(pl.multiple_of(lax.rem(q, per_own) * tile, tile), tile),
        )

    def owner(q):
        return lax.rem(t + 1 + q // per_own, T)

    def x_copy(q, to, src):
        return remote(
            comb.at[z, q], out.at[home(src, q)], x_s.at[q],
            x_r.at[lax.rem(q, per_own), src], tp=to,
        )

    def up_dest(k):
        return jnp.where(k < 2, Z - 2 + k, Z - 1 - k)

    def dest_of(k):
        d = jnp.where(k == Z - 1, 0, up_dest(k))
        return jnp.where(2 * z < Z, d, Z - 1 - d)

    def add(d, q, extra, e):
        here = comb[d, q].astype(jnp.float32)
        comb[d, q] = (here + extra[e, q].astype(jnp.float32)).astype(comb.dtype)

    def compute(d, q, slot):
        tokens = tokens_of(d)
        factor = jnp.concatenate([weight[tokens]] * (tile // weight.shape[1]), axis=1)
        weights = down[
            pl.ds(pl.multiple_of(owner(q) * inner, inner), inner),
            pl.ds(pl.multiple_of(lax.rem(q, per_own) * tile, tile), tile),
        ]
        value = jnp.dot(hidden[tokens], weights, preferred_element_type=jnp.float32)
        pair[slot] = (value * factor).astype(comb.dtype).reshape(2, part, tile)
        pair_copy(d, q, slot).start()

    def paired(d, q, slot):
        pair_copy(d, q, slot).wait()
        here = pair[slot, core].astype(jnp.float32)
        comb[d, q] = (here + got[d, q].astype(jnp.float32)).astype(comb.dtype)

        @pl.when(jnp.logical_and(z == 0, d > z))
        def _():
            up_copy(d, q).start()

        @pl.when(jnp.logical_and(z == Z - 1, d < z))
        def _():
            dn_copy(d, q).start()

    late = 2
    edge = jnp.logical_or(z == 0, z == Z - 1)

    def partials(low, high):
        @pl.loop(low, high + late)
        def _(n):
            @pl.when(n < high)
            def _():
                compute(dest_of(n // parts), lax.rem(n, parts), lax.rem(n, 4))

            @pl.when(n >= low + late)
            def _():
                k = n - late
                paired(dest_of(k // parts), lax.rem(k, parts), lax.rem(k, 4))

    def settle_down():
        own_scale.wait()

        @pl.loop(1, F)
        def _(s):
            to = lax.rem(f + s, F)
            scale_copy(to, to).wait_recv()

        @pl.loop(0, F)
        def _(src):
            weight[pl.ds(pl.multiple_of(src * part, part), part)] = column(scale[src])

        settle(2)

    @pl.loop(1, Z)
    def _(d):
        low, high = z - d, z + d

        @pl.when(d == Z - 1)
        def _():
            settle_down()
            pl.when(edge)(lambda: partials(0, parts))

        pl.when(low >= 0)(lambda: partner_tokens(low))
        pl.when(high < Z)(lambda: partner_tokens(high))

        @pl.loop(0, chunks)
        def _(q):
            pl.when(d + 1 < Z)(lambda: chain(d + 1, q))

            @pl.when(d == 1)
            def _():
                span(q, chunks, lag)(lambda r: second(2, far - lag + r))

            @span(q, chunks, tiles)
            def _(i):
                pl.when(low >= 0)(lambda: hidden_tile(low, i))
                pl.when(high < Z)(lambda: hidden_tile(high, i))

    partials(jnp.where(edge, parts, 0), Z * parts)

    ups, downs = 2 * z, 2 * (Z - 1 - z)
    def turn(rank):
        first_two = rank - (Z - 2)
        return jnp.where(first_two >= 0, first_two, Z - 1 - rank) * parts + 2 * rank

    last = jnp.maximum(jnp.where(lower, turn(z), 0), jnp.where(upper, turn(Z - 1 - z), 0))

    @pl.loop(0, Z * parts + 2 * Z)
    def _(step):
        u, v, w = step - ups, step - downs, step - last
        uq, vq = lax.rem(jnp.maximum(u, 0), parts), lax.rem(jnp.maximum(v, 0), parts)
        high = up_dest(jnp.maximum(u, 0) // parts)
        low = Z - 1 - up_dest(jnp.maximum(v, 0) // parts)
        going = (Z - 1) * parts

        @pl.when(lower & (u >= 0) & (u < going) & (high >= z))
        def _():
            up_copy(high, uq).wait_recv()
            add(high, uq, above, high)

            @pl.when(high > z)
            def _():
                up_copy(high, uq).start()

        @pl.when(upper & (v >= 0) & (v < going) & (low <= z))
        def _():
            dn_copy(low, vq).wait_recv()
            add(low, vq, above, jnp.where(low == z, Z, low))

            @pl.when(low < z)
            def _():
                dn_copy(low, vq).start()

        @pl.when(jnp.logical_and(w >= 0, w < parts))
        def _():
            @pl.when(w < parts - per_own)
            def _():
                x_copy(w, owner(w), t).start()

            @pl.when(w >= parts - per_own)
            def _():
                out[home(t, w)] = comb[z, w]

    @pl.loop(0, Z)
    def _(d):
        @pl.loop(0, parts)
        def _(q):
            @pl.when(jnp.logical_and(upper, d > z))
            def _():
                up_copy(d, q).wait_send()

            @pl.when(jnp.logical_and(lower, d < z))
            def _():
                dn_copy(d, q).wait_send()

    @pl.loop(0, parts - per_own)
    def _(q):
        x_copy(q, owner(q), t).wait_send()
        x_copy(q, owner(q), owner(q)).wait_recv()

    for m in range(3):
        sent = mats[m][1].at[pl.ds(0, mats[m][1].shape[0] - mats[m][0].shape[1])]
        remote(sent, sent, send_w.at[m], recv_w.at[m, 0, 0, 0], fs=partner).wait_send()

    @pl.loop(1, F)
    def _(s):
        scale_copy(lax.rem(f + s, F), f).wait_send()

    @pl.loop(0, Z)
    def _(d):
        src = 2 * d + core

        @pl.loop(0, chunks)
        def _(q):
            token_copy(token_rows(src, q), src, q, 2).wait_send()

            @pl.when(jnp.logical_and(d <= z, upper))
            def _():
                token_copy(token_rows(src, q), src, q, 0).wait_send()

            @pl.when(jnp.logical_and(d >= z, lower))
            def _():
                token_copy(token_rows(src, q), src, q, 1).wait_send()


def deliver(T, gate, up, down, mixed, gate_out, up_out, down_out, mixed_out, sems):
    t = lax.axis_index("tp")
    depth, own, width = gate_out.shape[1], down_out.shape[1], down.shape[1]
    deep = pl.ds(pl.multiple_of(t * depth, depth), depth)
    copies = [
        pltpu.make_async_copy(gate.at[deep], gate_out.at[0], sems.at[0]),
        pltpu.make_async_copy(up.at[deep], up_out.at[0], sems.at[1]),
        pltpu.make_async_copy(mixed, mixed_out, sems.at[2]),
    ]
    for tt in range(T):
        source = down.at[pl.ds(pl.multiple_of((tt * T + t) * own, own), own)]
        copies.append(
            pltpu.make_async_copy(
                source, down_out.at[0, :, pl.ds(tt * width, width)], sems.at[3 + tt]
            )
        )
    for copy in copies:
        copy.start()
    for copy in copies:
        copy.wait()


def shards(mesh, prompt, routes, route_weight, norm_gain, gate_train, up_train, down_train):
    G, F, T = (mesh.shape[name] for name in ("grp", "fs", "tp"))
    Z = F // 2
    t = lax.axis_index("tp")
    experts = gate_train.shape[0]
    tok_rows, width = prompt.shape
    part = tok_rows // T
    lanes = jnp.arange(experts, dtype=jnp.int32)
    routes = lax.dynamic_slice_in_dim(routes, t * part, part, 0)
    route_weight = lax.dynamic_slice_in_dim(route_weight, t * part, part, 0)
    scale = jnp.sum(
        jnp.where(routes[:, :, None] == lanes[None, None, :], route_weight[:, :, None], 0.0), axis=1
    )

    scale = scale.T.reshape(experts, 1, part)
    mats = (gate_train, up_train, down_train)
    full = [jax.ShapeDtypeStruct((T * F * w.shape[1], w.shape[2]), jnp.bfloat16) for w in mats]
    mixed = jax.ShapeDtypeStruct((tok_rows, width // T), jnp.bfloat16)
    inner = T * mats[0].shape[2]
    tile = min(512, width // T)
    parts = width // tile
    chunks = part // chunk_rows(part)
    bf16, f32, dma = jnp.bfloat16, jnp.float32, pltpu.SemaphoreType.DMA
    slots = min(4, F)
    scratch = F * part * (5 * width + 2 * inner + 512) + part * width * 6
    scratch += sum(2 * w.size + 4 * slots * w[0].size for w in mats)
    results = 2 * sum(w.size for w in full + [mixed])
    room = scratch + 6 * 1024 * 1024
    if room + results > 56 * 1024 * 1024:
        room += results
    held = pl.pallas_call(
        functools.partial(layer, (G, F, T)),
        out_shape=full + [mixed],
        in_specs=[pl.BlockSpec(memory_space=pl.ANY)] * 2
        + [pl.BlockSpec(memory_space=pltpu.VMEM)]
        + [pl.BlockSpec(memory_space=pl.ANY)] * 3,
        out_specs=[pl.BlockSpec(memory_space=pltpu.VMEM)] * 4,
        scratch_shapes=[
            pltpu.VMEM((F * part, width), bf16),
            pltpu.VMEM((F * part, inner), bf16),
            pltpu.VMEM((Z, parts, part, tile), bf16),
            pltpu.VMEM((4, 2, part, tile), bf16),
            pltpu.VMEM((Z, parts, part, tile), bf16),
            pltpu.VMEM((Z + 1, parts, part, tile), bf16),
            pltpu.VMEM((F, 1, part), f32),
            pltpu.VMEM((F * part, 128), f32),
            pltpu.VMEM((mats[0].shape[1], 128), f32),
            *[pltpu.VMEM(w.shape, bf16) for w in mats],
            *[pltpu.VMEM((slots,) + w.shape[1:], f32) for w in mats],
            dma((3, slots)),
            dma((3, F, G, T)),
            dma((3,)),
            dma((F, chunks)),
            dma((F, chunks)),
            dma((F, chunks)),
            dma((F, chunks)),
            dma((F,)),
            dma((F,)),
            dma((2,)),
            dma((4,)),
            dma((Z, parts)),
            dma((Z, parts)),
            dma((Z, parts)),
            dma((Z, parts)),
            dma((Z, parts)),
            dma((parts,)),
            dma((parts // T, T)),
        ],
        compiler_params=pltpu.CompilerParams(
            collective_id=0, has_side_effects=True, vmem_limit_bytes=min(room, 63 * 1024 * 1024)
        ),
    )(scale, prompt, norm_gain.reshape(1, -1), *mats)
    return pl.pallas_call(
        functools.partial(deliver, T),
        out_shape=[
            jax.ShapeDtypeStruct((1, full[0].shape[0] // T, full[0].shape[1]), bf16),
            jax.ShapeDtypeStruct((1, full[1].shape[0] // T, full[1].shape[1]), bf16),
            jax.ShapeDtypeStruct((1, inner // T, width), bf16),
            mixed,
        ],
        in_specs=[pl.BlockSpec(memory_space=pl.ANY)] * 4,
        out_specs=[pl.BlockSpec(memory_space=pl.ANY)] * 4,
        scratch_shapes=[dma((3 + T,))],
        compiler_params=pltpu.CompilerParams(vmem_limit_bytes=1024 * 1024),
    )(*held)


def solution(mesh):
    return jax.shard_map(
        functools.partial(shards, mesh),
        mesh=mesh,
        in_specs=(
            P(("grp", "fs"), None),
            P(("grp", "fs"), None),
            P(("grp", "fs"), None),
            P("fs"),
            P(None, "fs", "tp"),
            P(None, "fs", "tp"),
            P(None, "fs", "tp"),
        ),
        out_specs=(
            P(("grp", "fs"), None, "tp"),
            P(("grp", "fs"), None, "tp"),
            P(("grp", "fs"), "tp", None),
            P(("grp", "fs"), "tp"),
        ),
        check_vma=False,
    )
```

```python
import functools

import jax
import jax.numpy as jnp
from jax import lax
from jax.experimental import pallas as pl
from jax.experimental.pallas import tpu as pltpu
from jax.sharding import PartitionSpec as P

LIMIT = 7.0
ALPHA = 1.702
EPS = 1e-06
MESH = pl.DeviceIdType.MESH


def chunk_rows(rows):
    return 48 if rows % 48 == 0 else rows


def layer(
    sizes,
    scale_in,
    prompt,
    gain_in,
    gate_in,
    up_in,
    down_in,
    gate,
    up,
    down,
    out,
    tok,
    hidden,
    comb,
    pair,
    got,
    above,
    scale,
    weight,
    gain,
    ready_g,
    ready_u,
    ready_d,
    raw_g,
    raw_u,
    raw_d,
    raw_s,
    recv_w,
    send_w,
    recv_t,
    send_up,
    send_dn,
    send_pt,
    recv_s,
    send_s,
    local,
    pair_s,
    pair_r,
    up_s,
    up_r,
    dn_s,
    dn_r,
    x_s,
    x_r,
):
    G, F, T = sizes
    g, f, t = lax.axis_index("grp"), lax.axis_index("fs"), lax.axis_index("tp")
    Z = F // 2
    z, core = f // 2, lax.rem(f, 2)
    partner = f + 1 - 2 * core
    lower, upper = z > 0, z < Z - 1
    part, width = tok.shape[0] // F, tok.shape[1]
    own = width // T
    rows = chunk_rows(part)
    chunks = part // rows
    inner = hidden.shape[1]
    tile = got.shape[3]
    parts = width // tile
    per_own = own // tile
    cols = gate.shape[1]
    strips = min(256, cols)
    tiles = inner // strips
    far = F - 2
    lag = far // 2

    barrier = pltpu.get_barrier_semaphore()
    for axis, here, count in (("fs", f, F), ("grp", g, G), ("tp", t, T)):
        for s in range(1, count):
            pl.semaphore_signal(
                barrier, inc=1, device_id={axis: lax.rem(here + s, count)}, device_id_type=MESH
            )
    pl.semaphore_wait(barrier, F + G + T - 3)

    def remote(src, dst, send, recv, **where):
        return pltpu.make_async_remote_copy(
            src_ref=src, dst_ref=dst, send_sem=send, recv_sem=recv, device_id=where,
            device_id_type=MESH,
        )

    mats = ((ready_g, gate), (ready_u, up), (ready_d, down))
    trained = ((gate_in, raw_g), (up_in, raw_u), (down_in, raw_d))
    slots = raw_g.shape[0]

    def block_rows(m, src, tt):
        block = mats[m][0].shape[1]
        return mats[m][1].at[pl.ds(pl.multiple_of((tt * F + src) * block, block), block)]

    def piece_rows(m, src, gg, tt):
        block = mats[m][0].shape[1]
        piece = block // G
        start = (tt * F + src) * block + gg * piece
        return mats[m][1].at[pl.ds(pl.multiple_of(start, piece), piece)]

    def sent_piece(m, expert):
        piece = mats[m][0].shape[1] // G
        return mats[m][0].at[expert, pl.ds(pl.multiple_of(g * piece, piece), piece)]

    def wait_piece(m, src, gg, tt):
        ref = piece_rows(m, src, gg, tt)
        remote(ref, ref, send_w.at[m], recv_w.at[m, src, gg, tt], fs=partner).wait_recv()

    def pass_piece(m, src, gg, tt, **where):
        ref = piece_rows(m, src, gg, tt)
        remote(ref, ref, send_w.at[m], recv_w.at[m, src, gg, tt], **where).start()

    def wait_block(m, src, tt):
        ref = block_rows(m, src, tt)
        remote(ref, ref, send_w.at[m], recv_w.at[m, src, 0, tt], fs=partner).wait_recv()

    def near_blocks(m, src_ref, src):
        for dt in range(1, T):
            remote(
                src_ref, block_rows(m, src, t), send_w.at[m], recv_w.at[m, src, 0, t],
                tp=lax.rem(t + dt, T),
            ).start()

    both = jnp.minimum(z, Z - 1 - z)
    rising = jnp.where(2 * z < Z, 1, -1)

    def far_peer(r):
        k, side = r // 2, lax.rem(r, 2)
        near = (k // 2 + 1) * (2 * lax.rem(k, 2) - 1)
        chip = z + rising * jnp.where(k < 2 * both, near, k - both + 1)
        return 2 * chip + jnp.where(side == 0, core, 1 - core)

    def token_block(src):
        return tok.at[pl.ds(pl.multiple_of(src * part, part), part)]

    def token_rows(src, q):
        return tok.at[pl.ds(pl.multiple_of(src * part + q * rows, rows), rows)]

    own_tokens = pltpu.make_async_copy(
        prompt.at[pl.ds(pl.multiple_of(t * part, part), part)], token_block(f), local.at[0]
    )
    own_scale = pltpu.make_async_copy(scale_in.at[f], scale.at[f], local.at[1])

    def scale_copy(to, src):
        return remote(scale_in.at[to], scale.at[src], send_s.at[to], recv_s.at[src], fs=to)

    def token_copy(src_ref, src, q, kind):
        sems, to = ((send_up, f + 2), (send_dn, f - 2), (send_pt, partner))[kind]
        return remote(src_ref, token_rows(src, q), sems.at[src, q], recv_t.at[src, q], fs=to)

    def column(values):
        size = values.shape[1]
        row = lax.broadcasted_iota(jnp.int32, (size, size), 0)
        lane = lax.broadcasted_iota(jnp.int32, (size, size), 1)
        spread = jnp.where(row == lane, values, 0.0)
        return jnp.broadcast_to(jnp.sum(spread, axis=1, keepdims=True), (size, 128))

    def expert_of(i):
        return jnp.where(i == 0, partner, jnp.where(i == 1, f, far_peer(jnp.maximum(i - 2, 0))))

    def load(m, i):
        slot = lax.rem(i, slots)
        return pltpu.make_async_copy(
            trained[m][0].at[expert_of(i)], trained[m][1].at[slot], raw_s.at[m, slot]
        )

    for m in range(3):
        pl.loop(0, min(slots, F))(lambda i, m=m: load(m, i).start())

    def convert(m, i):
        load(m, i).wait()
        value = trained[m][1][lax.rem(i, slots)]
        if m < 2:
            value = value * jnp.concatenate([gain[...]] * (value.shape[1] // 128), axis=1)
        value = value.astype(mats[m][0].dtype)
        mats[m][0][expert_of(i)] = value
        block = value.shape[0]

        @pl.when(i == 1)
        def _():
            start = pl.multiple_of((t * F + f) * block, block)
            mats[m][1][pl.ds(start, block)] = value

        pl.when(i + slots < F)(lambda: load(m, i + slots).start())

    def send_piece(m, r):
        to = far_peer(r)
        remote(
            sent_piece(m, to), piece_rows(m, f, g, t), send_w.at[m], recv_w.at[m, f, g, t], fs=to
        ).start()

    def emit(m, i):
        @pl.when(i == 0)
        def _():
            remote(
                mats[m][0].at[partner], block_rows(m, f, t), send_w.at[m], recv_w.at[m, f, 0, t],
                fs=partner,
            ).start()

        if m == 0:
            pl.when(i == 1)(lambda: near_blocks(0, mats[0][0].at[f], f))
            pl.when(i > 1)(lambda: send_piece(m, i - 2))

    def send_tokens(q):
        source = token_rows(f, q)
        pl.when(upper)(lambda: token_copy(source, f, q, 0).start())
        pl.when(lower)(lambda: token_copy(source, f, q, 1).start())
        token_copy(source, f, q, 2).start()

    own_scale.start()
    own_tokens.start()

    @pl.loop(1, F)
    def _(s):
        scale_copy(lax.rem(f + s, F), f).start()

    gain[...] = column(gain_in[...])
    for m in range(3):

        @pl.loop(0, F + 1)
        def _(i, m=m):
            pl.when(i < F)(lambda: convert(m, i))
            pl.when(i > 0)(lambda: emit(m, i - 1))

    own_tokens.wait()

    @pl.loop(0, chunks)
    def _(q):
        where = pl.ds(pl.multiple_of(f * part + q * rows, rows), rows)
        values = tok[where].astype(jnp.float32)
        mean = jnp.mean(values * values, axis=-1, keepdims=True)
        tok[where] = (values * lax.rsqrt(mean + EPS)).astype(tok.dtype)

    def first(m, r):
        src = far_peer(r)
        wait_piece(m, src, g, t)
        for dg in range(1, G):
            pass_piece(m, src, g, t, grp=lax.rem(g + dg, G))
        for dt in range(1, T):
            pass_piece(m, src, g, t, tp=lax.rem(t + dt, T))

    def second(m, r):
        src = far_peer(r)
        across = lax.rem(r, 6) == 0
        for dg in range(1, G):
            gg = lax.rem(g + dg, G)
            wait_piece(m, src, gg, t)

            @pl.when(across)
            def _():
                for dt in range(1, T):
                    pass_piece(m, src, gg, t, tp=lax.rem(t + dt, T))

        for dt in range(1, T):
            tt = lax.rem(t + dt, T)
            wait_piece(m, src, g, tt)

            @pl.when(jnp.logical_not(across))
            def _():
                for dg in range(1, G):
                    pass_piece(m, src, g, tt, grp=lax.rem(g + dg, G))

    def settle(m):
        @pl.loop(0, far)
        def _(r):
            for dg in range(1, G):
                for dt in range(1, T):
                    wait_piece(m, far_peer(r), lax.rem(g + dg, G), lax.rem(t + dt, T))

        for src in (f, partner):
            for dt in range(1, T):
                wait_block(m, src, lax.rem(t + dt, T))

    def chain(d, q):
        @pl.when(z >= d)
        def _():
            src = f - 2 * d
            token_copy(token_rows(src, q), src, q, 2).wait_recv()

            @pl.when(upper)
            def _():
                token_copy(token_rows(src, q), src, q, 0).start()

            token_copy(token_rows(src, q), src, q, 2).start()

        @pl.when(z + d < Z)
        def _():
            src = f + 2 * d
            token_copy(token_rows(src, q), src, q, 2).wait_recv()

            @pl.when(lower)
            def _():
                token_copy(token_rows(src, q), src, q, 1).start()

            token_copy(token_rows(src, q), src, q, 2).start()

    def tokens_of(d):
        return pl.ds(pl.multiple_of(d * 2 * part, 2 * part), 2 * part)

    def partner_tokens(d):
        src = 2 * d + 1 - core

        @pl.loop(0, chunks)
        def _(q):
            token_copy(token_rows(src, q), src, q, 2).wait_recv()

    def hidden_tile(d, i):
        per = cols // strips
        tt, col = i // per, lax.rem(i, per) * strips
        where = (
            pl.ds(pl.multiple_of(tt * width, width), width),
            pl.ds(pl.multiple_of(col, strips), strips),
        )
        held = tok[tokens_of(d)]
        gate_pre = jnp.dot(held, gate[where], preferred_element_type=jnp.float32)
        up_pre = jnp.dot(held, up[where], preferred_element_type=jnp.float32)
        gate_pre = jnp.minimum(gate_pre, LIMIT)
        up_pre = jnp.clip(up_pre, -LIMIT, LIMIT)
        value = (up_pre + 1.0) * gate_pre * jax.nn.sigmoid(ALPHA * gate_pre)
        hidden[tokens_of(d), pl.ds(pl.multiple_of(i * strips, strips), strips)] = value.astype(
            hidden.dtype
        )

    def span(i, count, total):
        return pl.loop(i * total // count, (i + 1) * total // count)

    for m in range(3):
        if m > 0:
            near_blocks(m, mats[m][0].at[f], f)
        if m == 1:
            own_scale.wait()

            @pl.loop(1, F)
            def _(s):
                to = lax.rem(f + s, F)
                scale_copy(to, to).wait_recv()

            @pl.loop(0, F)
            def _(src):
                weight[pl.ds(pl.multiple_of(src * part, part), part)] = column(scale[src])

        if m == 2:
            pl.loop(far - lag, far)(lambda r: second(1, r))
            pl.loop(0, chunks)(lambda q: chain(1, q))

        @pl.loop(0, far)
        def _(r, m=m):
            first(m, r)
            if m == 0:
                send_piece(1, r)

            @pl.when(r >= lag)
            def _():
                second(m, r - lag)

            if m == 1:

                @pl.when(r < lag)
                def _():
                    second(m - 1, far - lag + r)

            if m == 1:

                @pl.when(r < lag)
                def _():
                    span(r, lag, chunks)(send_tokens)

                @pl.when(r >= lag)
                def _():
                    span(r - lag, far - lag, far)(lambda k: send_piece(2, k))

            if m == 2:

                @pl.when(r == lag)
                def _():
                    partner_tokens(z)
                    settle(0)
                    settle(1)

                @pl.when(r >= lag)
                def _():
                    span(r - lag, far - lag, tiles)(lambda i: hidden_tile(z, i))

        wait_block(m, partner, t)
        near_blocks(m, block_rows(m, partner, t), partner)

    def pair_copy(d, q, slot):
        return remote(
            pair.at[slot, 1 - core], got.at[d, q], pair_s.at[slot], pair_r.at[d, q], fs=partner
        )

    def up_copy(d, q):
        return remote(
            comb.at[d, q], above.at[d, q], up_s.at[d, q], up_r.at[d, q], fs=f + 2
        )

    def dn_copy(d, q):
        return remote(
            comb.at[d, q], above.at[jnp.where(d == z - 1, Z, d), q], dn_s.at[d, q],
            dn_r.at[d, q], fs=f - 2,
        )

    def home(src, q):
        return (
            pl.ds(pl.multiple_of(src * part, part), part),
            pl.ds(pl.multiple_of(lax.rem(q, per_own) * tile, tile), tile),
        )

    def owner(q):
        return lax.rem(t + 1 + q // per_own, T)

    def x_copy(q, to, src):
        return remote(
            comb.at[z, q], out.at[home(src, q)], x_s.at[q],
            x_r.at[lax.rem(q, per_own), src], tp=to,
        )

    def up_dest(k):
        return jnp.where(k < 2, Z - 2 + k, Z - 1 - k)

    def dest_of(k):
        d = jnp.where(k == Z - 1, 0, up_dest(k))
        return jnp.where(2 * z < Z, d, Z - 1 - d)

    def add(d, q, extra, e):
        here = comb[d, q].astype(jnp.float32)
        comb[d, q] = (here + extra[e, q].astype(jnp.float32)).astype(comb.dtype)

    def compute(d, q, slot):
        tokens = tokens_of(d)
        factor = jnp.concatenate([weight[tokens]] * (tile // weight.shape[1]), axis=1)
        weights = down[
            pl.ds(pl.multiple_of(owner(q) * inner, inner), inner),
            pl.ds(pl.multiple_of(lax.rem(q, per_own) * tile, tile), tile),
        ]
        value = jnp.dot(hidden[tokens], weights, preferred_element_type=jnp.float32)
        pair[slot] = (value * factor).astype(comb.dtype).reshape(2, part, tile)
        pair_copy(d, q, slot).start()

    def paired(d, q, slot):
        pair_copy(d, q, slot).wait()
        here = pair[slot, core].astype(jnp.float32)
        comb[d, q] = (here + got[d, q].astype(jnp.float32)).astype(comb.dtype)

        @pl.when(jnp.logical_and(z == 0, d > z))
        def _():
            up_copy(d, q).start()

        @pl.when(jnp.logical_and(z == Z - 1, d < z))
        def _():
            dn_copy(d, q).start()

    late = 2
    edge = jnp.logical_or(z == 0, z == Z - 1)

    def partials(low, high):
        @pl.loop(low, high + late)
        def _(n):
            @pl.when(n < high)
            def _():
                compute(dest_of(n // parts), lax.rem(n, parts), lax.rem(n, 4))

            @pl.when(n >= low + late)
            def _():
                k = n - late
                paired(dest_of(k // parts), lax.rem(k, parts), lax.rem(k, 4))

    @pl.loop(1, Z)
    def _(d):
        low, high = z - d, z + d

        @pl.when(d == Z - 1)
        def _():
            settle(2)
            pl.when(edge)(lambda: partials(0, parts))

        pl.when(low >= 0)(lambda: partner_tokens(low))
        pl.when(high < Z)(lambda: partner_tokens(high))

        @pl.loop(0, chunks)
        def _(q):
            pl.when(d + 1 < Z)(lambda: chain(d + 1, q))

            @pl.when(d == 1)
            def _():
                span(q, chunks, lag)(lambda r: second(2, far - lag + r))

            @span(q, chunks, tiles)
            def _(i):
                pl.when(low >= 0)(lambda: hidden_tile(low, i))
                pl.when(high < Z)(lambda: hidden_tile(high, i))

    partials(jnp.where(edge, parts, 0), Z * parts)

    ups, downs = 2 * z, 2 * (Z - 1 - z)
    def turn(rank):
        first_two = rank - (Z - 2)
        return jnp.where(first_two >= 0, first_two, Z - 1 - rank) * parts + 2 * rank

    last = jnp.maximum(jnp.where(lower, turn(z), 0), jnp.where(upper, turn(Z - 1 - z), 0))

    @pl.loop(0, Z * parts + 2 * Z)
    def _(step):
        u, v, w = step - ups, step - downs, step - last
        uq, vq = lax.rem(jnp.maximum(u, 0), parts), lax.rem(jnp.maximum(v, 0), parts)
        high = up_dest(jnp.maximum(u, 0) // parts)
        low = Z - 1 - up_dest(jnp.maximum(v, 0) // parts)
        going = (Z - 1) * parts

        @pl.when(lower & (u >= 0) & (u < going) & (high >= z))
        def _():
            up_copy(high, uq).wait_recv()
            add(high, uq, above, high)

            @pl.when(high > z)
            def _():
                up_copy(high, uq).start()

        @pl.when(upper & (v >= 0) & (v < going) & (low <= z))
        def _():
            dn_copy(low, vq).wait_recv()
            add(low, vq, above, jnp.where(low == z, Z, low))

            @pl.when(low < z)
            def _():
                dn_copy(low, vq).start()

        @pl.when(jnp.logical_and(w >= 0, w < parts))
        def _():
            @pl.when(w < parts - per_own)
            def _():
                x_copy(w, owner(w), t).start()

            @pl.when(w >= parts - per_own)
            def _():
                out[home(t, w)] = comb[z, w]

    @pl.loop(0, Z)
    def _(d):
        @pl.loop(0, parts)
        def _(q):
            @pl.when(jnp.logical_and(upper, d > z))
            def _():
                up_copy(d, q).wait_send()

            @pl.when(jnp.logical_and(lower, d < z))
            def _():
                dn_copy(d, q).wait_send()

    @pl.loop(0, parts - per_own)
    def _(q):
        x_copy(q, owner(q), t).wait_send()
        x_copy(q, owner(q), owner(q)).wait_recv()

    for m in range(3):
        sent = mats[m][1].at[pl.ds(0, mats[m][1].shape[0] - mats[m][0].shape[1])]
        remote(sent, sent, send_w.at[m], recv_w.at[m, 0, 0, 0], fs=partner).wait_send()

    @pl.loop(1, F)
    def _(s):
        scale_copy(lax.rem(f + s, F), f).wait_send()

    @pl.loop(0, Z)
    def _(d):
        src = 2 * d + core

        @pl.loop(0, chunks)
        def _(q):
            token_copy(token_rows(src, q), src, q, 2).wait_send()

            @pl.when(jnp.logical_and(d <= z, upper))
            def _():
                token_copy(token_rows(src, q), src, q, 0).wait_send()

            @pl.when(jnp.logical_and(d >= z, lower))
            def _():
                token_copy(token_rows(src, q), src, q, 1).wait_send()


def deliver(T, gate, up, down, mixed, gate_out, up_out, down_out, mixed_out, sems):
    t = lax.axis_index("tp")
    depth, own, width = gate_out.shape[1], down_out.shape[1], down.shape[1]
    deep = pl.ds(pl.multiple_of(t * depth, depth), depth)
    copies = [
        pltpu.make_async_copy(gate.at[deep], gate_out.at[0], sems.at[0]),
        pltpu.make_async_copy(up.at[deep], up_out.at[0], sems.at[1]),
        pltpu.make_async_copy(mixed, mixed_out, sems.at[2]),
    ]
    for tt in range(T):
        source = down.at[pl.ds(pl.multiple_of((tt * T + t) * own, own), own)]
        copies.append(
            pltpu.make_async_copy(
                source, down_out.at[0, :, pl.ds(tt * width, width)], sems.at[3 + tt]
            )
        )
    for copy in copies:
        copy.start()
    for copy in copies:
        copy.wait()


def shards(mesh, prompt, routes, route_weight, norm_gain, gate_train, up_train, down_train):
    G, F, T = (mesh.shape[name] for name in ("grp", "fs", "tp"))
    Z = F // 2
    t = lax.axis_index("tp")
    experts = gate_train.shape[0]
    tok_rows, width = prompt.shape
    part = tok_rows // T
    lanes = jnp.arange(experts, dtype=jnp.int32)
    routes = lax.dynamic_slice_in_dim(routes, t * part, part, 0)
    route_weight = lax.dynamic_slice_in_dim(route_weight, t * part, part, 0)
    scale = jnp.sum(
        jnp.where(routes[:, :, None] == lanes[None, None, :], route_weight[:, :, None], 0.0), axis=1
    )

    scale = scale.T.reshape(experts, 1, part)
    mats = (gate_train, up_train, down_train)
    full = [jax.ShapeDtypeStruct((T * F * w.shape[1], w.shape[2]), jnp.bfloat16) for w in mats]
    mixed = jax.ShapeDtypeStruct((tok_rows, width // T), jnp.bfloat16)
    inner = T * mats[0].shape[2]
    tile = min(512, width // T)
    parts = width // tile
    chunks = part // chunk_rows(part)
    bf16, f32, dma = jnp.bfloat16, jnp.float32, pltpu.SemaphoreType.DMA
    slots = min(4, F)
    scratch = F * part * (5 * width + 2 * inner + 512) + part * width * 6
    scratch += sum(2 * w.size + 4 * slots * w[0].size for w in mats)
    results = 2 * sum(w.size for w in full + [mixed])
    room = scratch + 6 * 1024 * 1024
    if room + results > 56 * 1024 * 1024:
        room += results
    held = pl.pallas_call(
        functools.partial(layer, (G, F, T)),
        out_shape=full + [mixed],
        in_specs=[pl.BlockSpec(memory_space=pl.ANY)] * 2
        + [pl.BlockSpec(memory_space=pltpu.VMEM)]
        + [pl.BlockSpec(memory_space=pl.ANY)] * 3,
        out_specs=[pl.BlockSpec(memory_space=pltpu.VMEM)] * 4,
        scratch_shapes=[
            pltpu.VMEM((F * part, width), bf16),
            pltpu.VMEM((F * part, inner), bf16),
            pltpu.VMEM((Z, parts, part, tile), bf16),
            pltpu.VMEM((4, 2, part, tile), bf16),
            pltpu.VMEM((Z, parts, part, tile), bf16),
            pltpu.VMEM((Z + 1, parts, part, tile), bf16),
            pltpu.VMEM((F, 1, part), f32),
            pltpu.VMEM((F * part, 128), f32),
            pltpu.VMEM((mats[0].shape[1], 128), f32),
            *[pltpu.VMEM(w.shape, bf16) for w in mats],
            *[pltpu.VMEM((slots,) + w.shape[1:], f32) for w in mats],
            dma((3, slots)),
            dma((3, F, G, T)),
            dma((3,)),
            dma((F, chunks)),
            dma((F, chunks)),
            dma((F, chunks)),
            dma((F, chunks)),
            dma((F,)),
            dma((F,)),
            dma((2,)),
            dma((4,)),
            dma((Z, parts)),
            dma((Z, parts)),
            dma((Z, parts)),
            dma((Z, parts)),
            dma((Z, parts)),
            dma((parts,)),
            dma((parts // T, T)),
        ],
        compiler_params=pltpu.CompilerParams(
            collective_id=0, has_side_effects=True, vmem_limit_bytes=min(room, 63 * 1024 * 1024)
        ),
    )(scale, prompt, norm_gain.reshape(1, -1), *mats)
    return pl.pallas_call(
        functools.partial(deliver, T),
        out_shape=[
            jax.ShapeDtypeStruct((1, full[0].shape[0] // T, full[0].shape[1]), bf16),
            jax.ShapeDtypeStruct((1, full[1].shape[0] // T, full[1].shape[1]), bf16),
            jax.ShapeDtypeStruct((1, inner // T, width), bf16),
            mixed,
        ],
        in_specs=[pl.BlockSpec(memory_space=pl.ANY)] * 4,
        out_specs=[pl.BlockSpec(memory_space=pl.ANY)] * 4,
        scratch_shapes=[dma((3 + T,))],
        compiler_params=pltpu.CompilerParams(vmem_limit_bytes=1024 * 1024),
    )(*held)


def solution(mesh):
    return jax.shard_map(
        functools.partial(shards, mesh),
        mesh=mesh,
        in_specs=(
            P(("grp", "fs"), None),
            P(("grp", "fs"), None),
            P(("grp", "fs"), None),
            P("fs"),
            P(None, "fs", "tp"),
            P(None, "fs", "tp"),
            P(None, "fs", "tp"),
        ),
        out_specs=(
            P(("grp", "fs"), None, "tp"),
            P(("grp", "fs"), None, "tp"),
            P(("grp", "fs"), "tp", None),
            P(("grp", "fs"), "tp"),
        ),
        check_vma=False,
    )
```
